32 devices in a mesh: ep: 8 (over z, x), tp: 4 (over y, core).
Axes of the slice: x: 2, y: 2, z: 4, core: 2. Of those that a mesh axis runs over, the one named last changes fastest.
Arguments:
- queries: bfloat16 [4096, 2048], P('ep', 'tp'), may hold values from -5 to 5
- key_rows: bfloat16 [4096, 2048], P('ep', 'tp'), may hold values from -5 to 5
- values: bfloat16 [4096, 2048], P('ep', 'tp'), may hold values from -6 to 6
- forget_log: float32 [4096, 16], P(None, 'tp'), may hold values from -515 to 0, as said below
- out_weight: bfloat16 [2048, 4096], P(None, 'tp'), may hold values from -1 to 1
- expert_input: bfloat16 [1024, 4096], P(('ep', 'tp')), may hold values from -6 to 6
- norm_gain: float32 [4096], replicated, may hold values from 0.1 to 1.9
- route_ids: int32 [1024, 2], P('ep'), may hold values from 0 to 7, all different within a row; in each aligned block of 128 rows (0 to 127, 128 to 255, ...) at most 64 rows name the same one
- route_weights: float32 [1024, 2], P('ep'), may hold values from 0.2 to 1
- gate_weight: bfloat16 [8, 4096, 2048], P('ep', None, 'tp'), may hold values from -0.09375 to 0.09375
- up_weight: bfloat16 [8, 4096, 2048], P('ep', None, 'tp'), may hold values from -0.09375 to 0.09375
- down_weight: bfloat16 [8, 2048, 4096], P('ep', None, 'tp'), may hold values from -0.125 to 0.125
Outputs:
- mixer_out: bfloat16 [4096, 4096], P('ep', 'tp')
- expert_out: bfloat16 [1024, 4096], P('ep', 'tp')
The draws below stay inside these ranges and needn't reach their ends.
Inputs may be any that keep to these rules, and one draw needn't show every extreme that they name: forget_log[t, h] is the sum of the log forget gates of head h at positions 0 to t of the one sequence; it never rises along positions. `route_ids`: each row names 2 different experts. In each aligned block of 128 rows (the rows of one index of ep) no expert is named by more than 64 rows, and some block reaches 64.
All inputs are finite; a program needn't handle non-finite values.
Results may differ from the reference program's by a relative error of at most 0.0071.
Values may be sent and summed in bfloat16 or wider, within the bound.
A program may use at most 64 MiB of HBM per device.

```python
import math
import jax
import jax.numpy as jnp
import numpy as np
from jax import lax

D = 4096
HEAD_COUNT = 16
HD = 128
FFE = 2048
TOPK = 2
ROWS_A = 512
ROWS_B = 128
SEQUENCE_LENGTH = 4096
TOKENS_B = 1024
EXPERTS = 8
CAP = 64
N_EP = 8


def draw_queries(key, part):
    drawn_rows = jnp.clip(1.5 * jax.random.normal(jax.random.fold_in(key, 1), (SEQUENCE_LENGTH, HEAD_COUNT * HD), jnp.float32), -5.0, 5.0)
    return drawn_rows.astype(jnp.bfloat16)


def draw_key_rows(key, part):
    drawn_rows = jnp.clip(jax.random.normal(jax.random.fold_in(key, 2), (SEQUENCE_LENGTH, HEAD_COUNT * HD), jnp.float32), -5.0, 5.0)
    return drawn_rows.astype(jnp.bfloat16)


def draw_forget_log(key, part):
    fast_share = 0.5
    fast_heads = jax.random.uniform(jax.random.fold_in(key, 3), (HEAD_COUNT,), jnp.float32) < fast_share
    slow_rate = jnp.exp(jax.random.uniform(jax.random.fold_in(key, 4), (HEAD_COUNT,), jnp.float32, jnp.log(0.2), jnp.log(0.8))) / SEQUENCE_LENGTH
    fast_rate = jnp.exp(jax.random.uniform(jax.random.fold_in(key, 5), (HEAD_COUNT,), jnp.float32, jnp.log(0.01), jnp.log(1.0 / 30.0)))
    head_rate = jnp.where(fast_heads, fast_rate, slow_rate)
    block_factor = jnp.exp(jax.random.uniform(jax.random.fold_in(key, 6), (SEQUENCE_LENGTH // ROWS_A, HEAD_COUNT), jnp.float32, -0.7, 0.7))
    block_factor = jnp.repeat(block_factor, ROWS_A, axis=0)
    roughness = jax.random.uniform(jax.random.fold_in(key, 7), (SEQUENCE_LENGTH, HEAD_COUNT), jnp.float32, 0.3, 1.7)
    step_logarithm = -head_rate[None, :] * block_factor * roughness
    surge_locations = jax.random.randint(jax.random.fold_in(key, 8), (2, HEAD_COUNT), 0, SEQUENCE_LENGTH)
    position_indices = jnp.arange(SEQUENCE_LENGTH, dtype=jnp.int32)
    surge_matched = jnp.any(position_indices[:, None, None] == surge_locations[None, :, :], axis=1)
    surge_penalty = jnp.log(jax.random.uniform(jax.random.fold_in(key, 9), (SEQUENCE_LENGTH, HEAD_COUNT), jnp.float32, 0.6, 0.8))
    step_logarithm = step_logarithm + jnp.where(surge_matched, surge_penalty, 0.0)
    return jnp.cumsum(step_logarithm, axis=0).astype(jnp.float32)


def block_scale(rng, extent, split, least, top_value):
    factor_of, own = 1.0, jax.random.fold_in(rng, 6)
    for dim, shards_of in split:
        draws = jnp.exp(jax.random.uniform(jax.random.fold_in(own, dim), (shards_of,), jnp.float32, least / len(split), top_value / len(split)))
        factor_of = factor_of * jnp.repeat(draws, extent[dim] // shards_of).reshape([-1 if axis == dim else 1 for axis in range(len(extent))])
    return factor_of


def shared_out(rng, own, number, rows, number_of, top, reach, skew):
    order = jax.random.permutation(rng, number_of)
    heavy_load, usual = load_shares(number_of, rows * top, reach, skew, True), load_shares(number_of, rows * top, reach, skew, False)
    places = jnp.arange(number_of)

    def named(sizes, offset_by):
        used = int((sizes > 0).sum())
        fixed = max(1, used // 4)
        passed = fixed + (places - fixed + offset_by * (used - fixed)) % max(1, number_of - fixed)
        return jnp.zeros((number_of,), jnp.int32).at[order[jnp.where(places < fixed, places, passed)]].set(jnp.asarray(sizes, jnp.int32))

    sizes = jnp.where(number % 4 == 0, named(heavy_load, number // 4), named(usual, number - number // 4 - 1))
    mixed = jax.random.permutation(jax.random.fold_in(own, 3), number_of)
    giver, receiver = mixed[0:number_of // 2 * 2:2], mixed[1:number_of // 2 * 2:2]
    slack = jnp.minimum(sizes[giver] - 1, reach - sizes[receiver]) // 2
    slack = jnp.where((giver == order[0]) | (receiver == order[0]) | (sizes[receiver] == 0), 0, jnp.maximum(slack, 0))
    passed = jax.random.randint(jax.random.fold_in(own, 4), (number_of // 2,), 0, 1 << 20) % (slack + 1)
    sizes = sizes.at[giver].add(-passed).at[receiver].add(passed)
    items = jnp.searchsorted(jnp.cumsum(sizes), jnp.arange(rows * top), side="right").astype(jnp.int32)
    table = items.reshape(top, rows).T
    table = table[jax.random.permutation(jax.random.fold_in(own, 1), rows)]
    offset_by = jax.random.randint(jax.random.fold_in(own, 2), (rows, 1), 0, top)
    return jnp.take_along_axis(table, (jnp.arange(top)[None, :] + offset_by) % top, axis=1)


def load_shares(count, total, limit, slope, full):
    portions = [(1 << 20) // math.isqrt(grade ** slope) + 1 for grade in range(1, count + 1)]
    largest = limit if full else min(limit, max(-(-total // count), total * portions[0] // sum(portions)))
    least = 1 if total - largest >= count - 1 else 0
    counts, rest = [largest] + [least] * (count - 1), total - largest - least * (count - 1)
    while rest > 0:
        movable = [i for i in range(1, count) if counts[i] < largest] or [i for i in range(1, count) if counts[i] < limit]
        mass, left = sum([portions[i] for i in movable]), rest
        for i in movable:
            addition = min(limit - counts[i], max(1, left * portions[i] // mass), rest)
            counts[i] = counts[i] + addition
            rest = rest - addition
    return np.array(counts)


def noise(key, dims, width, most, cuts=(), held_as=jnp.bfloat16):
    factor_of = block_scale(key, dims, cuts, -0.22, 0.18) if cuts else 1.0
    drawn = jax.random.normal(key, dims, jnp.float32) * width * factor_of
    return jnp.minimum(jnp.maximum(drawn, -most), most).astype(held_as)


def setup_inputs(seed: int = 0) -> dict:
    key_list = jax.random.split(jax.random.key(seed), 13)
    queries = draw_queries(jax.random.fold_in(key_list[12], 71), 0)
    key_rows = draw_key_rows(jax.random.fold_in(key_list[12], 71), 0)
    values = noise(key_list[2], (SEQUENCE_LENGTH, HEAD_COUNT * HD), 1.0, 6.0, ((0, 8), (1, 4)))
    forget_log = draw_forget_log(jax.random.fold_in(key_list[12], 71), 0)
    out_weight = noise(key_list[4], (HEAD_COUNT * HD, D), (HD // 4) ** -0.5, 1.0, ((1, 4),))
    expert_input = noise(key_list[5], (TOKENS_B, D), 1.0, 6.0, ((0, 32),))
    norm_gain = jnp.clip(1.0 + 0.18 * jax.random.normal(key_list[6], (D,), jnp.float32), 0.1, 1.9)
    route_ids_keys = jax.random.split(jax.random.fold_in(key_list[7], 1), TOKENS_B // ROWS_B)
    route_ids_turns = jax.random.permutation(jax.random.fold_in(key_list[7], 3), TOKENS_B // ROWS_B)
    route_ids = jax.vmap(lambda own, number: shared_out(jax.random.fold_in(key_list[7], 2), own, number, ROWS_B, EXPERTS, TOPK, CAP, 2))(route_ids_keys, route_ids_turns).reshape((TOKENS_B, TOPK))
    route_weights = jnp.clip(0.2 + 0.8 * jax.random.uniform(key_list[8], (TOKENS_B, TOPK), jnp.float32) ** block_scale(key_list[8], (TOKENS_B, TOPK), ((0, 8),), -0.2, 0.2), 0.2, 1.0)
    gate_weight = noise(key_list[9], (EXPERTS, D, FFE), D ** -0.5, 0.09375, ((0, 8), (2, 4)))
    up_weight = noise(key_list[10], (EXPERTS, D, FFE), D ** -0.5, 0.09375, ((0, 8), (2, 4)))
    down_weight = noise(key_list[11], (EXPERTS, FFE, D), FFE ** -0.5, 0.125, ((0, 8), (2, 4)))
    return {"queries": queries, "key_rows": key_rows, "values": values, "forget_log": forget_log, "out_weight": out_weight, "expert_input": expert_input, "norm_gain": norm_gain, "route_ids": route_ids, "route_weights": route_weights, "gate_weight": gate_weight, "up_weight": up_weight, "down_weight": down_weight}


EPSILON = 1e-05

def slot_places(route_rows, experts, capacity):
    entries = route_rows.reshape(-1).astype(jnp.int32)
    matches = (entries[:, None] == jnp.arange(experts, dtype=jnp.int32)[None, :]).astype(jnp.int32)
    earlier = (jnp.cumsum(matches, axis=0) - matches).astype(jnp.int32)
    ranking = lax.optimization_barrier(jnp.sum(earlier * matches, axis=1)).astype(jnp.int32)
    return (entries * capacity + ranking).astype(jnp.int32)

def reference(queries, key_rows, values, forget_log, out_weight, expert_input, norm_gain, route_ids, route_weights, gate_weight, up_weight, down_weight):
    length_all = queries.shape[0]
    query_heads = queries.reshape(length_all, HEAD_COUNT, HD).astype(jnp.float32)
    key_heads = key_rows.reshape(length_all, HEAD_COUNT, HD).astype(jnp.float32)
    value_heads = values.reshape(length_all, HEAD_COUNT, HD).astype(jnp.float32)
    key_places = jnp.arange(length_all, dtype=jnp.int32)
    score_scale = HD ** (-0.5)

    def attend(block_index):
        block_start = (block_index * ROWS_A).astype(jnp.int32)
        query_block = lax.dynamic_slice_in_dim(query_heads, block_start, ROWS_A, 0)
        gate_block = lax.dynamic_slice_in_dim(forget_log, block_start, ROWS_A, 0)
        scores = jnp.einsum('qhd,khd->hqk', query_block, key_heads) * score_scale
        scores = scores + gate_block.T[:, :, None] - forget_log.T[:, None, :]
        query_places = block_start + jnp.arange(ROWS_A, dtype=jnp.int32)
        scores = jnp.where(key_places[None, None, :] <= query_places[None, :, None], scores, -jnp.inf)
        row_max = lax.optimization_barrier(jnp.max(scores, axis=2, keepdims=True))
        weights_now = jnp.exp(scores - row_max)
        denominator = lax.optimization_barrier(jnp.sum(weights_now, axis=2))
        rounded = lax.optimization_barrier(weights_now.astype(jnp.bfloat16)).astype(jnp.float32)
        numerator = jnp.einsum('hqk,khd->qhd', rounded, value_heads)
        return (numerator / denominator.T[:, :, None]).astype(jnp.bfloat16)
    attended = lax.map(attend, jnp.arange(length_all // ROWS_A, dtype=jnp.int32)).reshape(length_all, HEAD_COUNT * HD)
    mixer_out = jnp.dot(attended, out_weight, preferred_element_type=jnp.float32).astype(jnp.bfloat16)
    as_float = expert_input.astype(jnp.float32)
    center = lax.optimization_barrier(jnp.mean(as_float, axis=1, keepdims=True))
    variance = lax.optimization_barrier(jnp.mean(jnp.square(as_float - center), axis=1, keepdims=True))
    normed = ((as_float - center) * lax.rsqrt(variance + EPSILON) * norm_gain).astype(jnp.bfloat16)
    blocks = route_ids.reshape(N_EP, ROWS_B, TOPK)
    places = jax.vmap(lambda block_ids: slot_places(block_ids, EXPERTS, CAP))(blocks)
    expert_of = blocks.reshape(N_EP, ROWS_B * TOPK).astype(jnp.int32)
    ranking = places - expert_of * CAP
    block_index = jnp.arange(N_EP, dtype=jnp.int32)[:, None]
    global_slot = (expert_of * (N_EP * CAP) + block_index * CAP + ranking).astype(jnp.int32)
    owners = (block_index * ROWS_B + jnp.arange(ROWS_B * TOPK, dtype=jnp.int32)[None, :] // TOPK).astype(jnp.int32)
    slot_table = jnp.full((EXPERTS * N_EP * CAP,), TOKENS_B, jnp.int32).at[global_slot.reshape(-1)].set(owners.reshape(-1))
    slot_table = slot_table.reshape(EXPERTS, N_EP * CAP)

    def run_expert(expert_index):
        chosen_rows = jnp.take(normed, slot_table[expert_index], axis=0, mode='fill', fill_value=0)
        gate_part = jnp.dot(chosen_rows, gate_weight[expert_index], preferred_element_type=jnp.float32)
        up_part = jnp.dot(chosen_rows, up_weight[expert_index], preferred_element_type=jnp.float32)
        hidden = (jax.nn.silu(gate_part) * up_part).astype(jnp.bfloat16)
        return jnp.dot(hidden, down_weight[expert_index], preferred_element_type=jnp.float32).astype(jnp.bfloat16)
    results = lax.map(run_expert, jnp.arange(EXPERTS, dtype=jnp.int32)).reshape(EXPERTS * N_EP * CAP, D)
    picked = jnp.take(results, global_slot.reshape(-1), axis=0).astype(jnp.float32)
    combined = lax.optimization_barrier(jnp.sum((picked * route_weights.reshape(-1)[:, None]).reshape(TOKENS_B, TOPK, D), axis=1))
    return (mixer_out, combined.astype(jnp.bfloat16))
```

```python
import functools
import math

import jax
import jax.numpy as jnp
from jax import lax
from jax.experimental import pallas as pl
from jax.experimental.pallas import tpu as pltpu
from jax.sharding import PartitionSpec as P

EPSILON = 1e-05
LOG2E = math.log2(math.e)


def attention_kernel(
    n, tp, heads, gate_row, gate_col, q_ref, k_ref, v_ref, pick_ref, token_ref,
    out_ref, routed_ref,
    k_buf, v_buf, q_buf, o_buf, token_buf, leave_buf,
    recv_k, recv_v, recv_q, recv_o, send_k, send_v, send_q, send_o, pass_k, pass_v,
    send_t, recv_t, send_a, recv_a, send_f, recv_f,
):
    members = n // heads
    rows = k_ref.shape[0]
    width = k_ref.shape[1] // heads
    chunk = rows // members
    me = lax.axis_index("ep")
    my_member = me % members
    my_head = me // members
    my_tp = lax.axis_index("tp")
    tokens = token_ref.shape[0]

    barrier = pltpu.get_barrier_semaphore()

    @pl.loop(1, n)
    def _(step):
        pl.semaphore_signal(barrier, inc=1, device_id={"ep": (me + step) % n})

    @pl.loop(1, tp)
    def _(step):
        pl.semaphore_signal(barrier, inc=1, device_id={"tp": (my_tp + step) % tp})

    pl.semaphore_wait(barrier, n + tp - 2)

    def k_copy(target, head):
        cols = pl.ds(pl.multiple_of(head * width, width), width)
        return pltpu.make_async_remote_copy(
            src_ref=k_ref.at[:, cols], dst_ref=k_buf.at[me], send_sem=send_k.at[head],
            recv_sem=recv_k.at[me], device_id={"ep": target},
        )

    def v_copy(target, head):
        cols = pl.ds(pl.multiple_of(head * width, width), width)
        return pltpu.make_async_remote_copy(
            src_ref=v_ref.at[:, cols], dst_ref=v_buf.at[me], send_sem=send_v.at[head],
            recv_sem=recv_v.at[me], device_id={"ep": target},
        )

    def q_copy(target):
        cols = pl.ds(pl.multiple_of((target // members) * width, width), width)
        part = pl.ds(pl.multiple_of((target % members) * chunk, chunk), chunk)
        return pltpu.make_async_remote_copy(
            src_ref=q_ref.at[part, cols], dst_ref=q_buf.at[me], send_sem=send_q.at[target],
            recv_sem=recv_q.at[me], device_id={"ep": target},
        )

    def pass_copies(source, target):
        return (
            pltpu.make_async_remote_copy(
                src_ref=k_buf.at[source], dst_ref=k_buf.at[source],
                send_sem=pass_k.at[source, target % members],
                recv_sem=recv_k.at[source], device_id={"ep": target},
            ),
            pltpu.make_async_remote_copy(
                src_ref=v_buf.at[source], dst_ref=v_buf.at[source],
                send_sem=pass_v.at[source, target % members],
                recv_sem=recv_v.at[source], device_id={"ep": target},
            ),
        )

    def back_copy(source):
        cols = pl.ds(pl.multiple_of(my_head * width, width), width)
        part = pl.ds(pl.multiple_of(my_member * chunk, chunk), chunk)
        return pltpu.make_async_remote_copy(
            src_ref=o_buf.at[source], dst_ref=out_ref.at[part, cols], send_sem=send_o.at[source],
            recv_sem=recv_o.at[me], device_id={"ep": source},
        )

    def token_spot(owner):
        return token_buf.at[pl.ds(pl.multiple_of(owner * tokens, tokens), tokens), :]

    def token_copy(target):
        return pltpu.make_async_remote_copy(
            src_ref=token_ref, dst_ref=token_spot(my_tp), send_sem=send_t.at[target],
            recv_sem=recv_t.at[my_tp], device_id={"tp": target},
        )

    def leave_copy(target):
        return pltpu.make_async_remote_copy(
            src_ref=leave_buf.at[target], dst_ref=routed_ref.at[me, my_tp],
            send_sem=send_a.at[target], recv_sem=recv_a.at[me], device_id={"ep": target},
        )

    def spread_copy(source, target):
        spot = routed_ref.at[source, my_tp]
        return pltpu.make_async_remote_copy(
            src_ref=spot, dst_ref=spot, send_sem=send_f.at[source, target],
            recv_sem=recv_f.at[source, my_tp], device_id={"tp": target},
        )

    pltpu.make_async_copy(token_ref, token_spot(my_tp), recv_t.at[my_tp]).start()

    @pl.loop(1, tp)
    def _(step):
        token_copy((my_tp + step) % tp).start()

    own_cols = pl.ds(pl.multiple_of(my_head * width, width), width)
    own_part = pl.ds(pl.multiple_of(my_member * chunk, chunk), chunk)
    pltpu.make_async_copy(k_ref.at[:, own_cols], k_buf.at[me], recv_k.at[me]).start()
    pltpu.make_async_copy(v_ref.at[:, own_cols], v_buf.at[me], recv_v.at[me]).start()
    pltpu.make_async_copy(q_ref.at[own_part, own_cols], q_buf.at[me], recv_q.at[me]).start()

    @pl.loop(1, heads)
    def _(step):
        head = (my_head + step) % heads
        k_copy(head * members + my_member, head).start()
        v_copy(head * members + my_member, head).start()

    @pl.loop(1, n)
    def _(step):
        q_copy((me + step) % n).start()

    @pl.loop(0, tp)
    def _(owner):
        pltpu.make_async_copy(token_spot(owner), token_spot(owner), recv_t.at[owner]).wait()

    @pl.loop(0, n)
    def _(target):
        leave_buf[target] = jnp.dot(
            pick_ref[target], token_buf[...], preferred_element_type=jnp.float32
        ).astype(leave_buf.dtype)

    pltpu.make_async_copy(leave_buf.at[me], routed_ref.at[me, my_tp], recv_a.at[me]).start()

    @pl.loop(1, n)
    def _(step):
        leave_copy((me + step) % n).start()

    def landed(source):
        pltpu.make_async_copy(k_buf.at[source], k_buf.at[source], recv_k.at[source]).wait()
        pltpu.make_async_copy(v_buf.at[source], v_buf.at[source], recv_v.at[source]).wait()

    @pl.loop(0, heads)
    def _(step):
        source = ((my_head + step) % heads) * members + my_member
        landed(source)

        @pl.loop(1, members)
        def _(other):
            for copy in pass_copies(source, my_head * members + (my_member + other) % members):
                copy.start()

    column = lax.broadcasted_iota(jnp.int32, (chunk, rows), 1)
    line = lax.broadcasted_iota(jnp.int32, (chunk, rows), 0) + my_member * chunk
    causal = column <= line
    factor = LOG2E * width ** (-0.5)

    @pl.loop(0, n)
    def _(i):
        pltpu.make_async_copy(q_buf.at[i], q_buf.at[i], recv_q.at[i]).wait()

        @pl.when(i % members != my_member)
        def _():
            landed(i)

        query = q_buf[i]
        line_gate = gate_col[i]

        def scores_of(j):
            raw = lax.dot_general(
                query, k_buf[j], (((1,), (1,)), ((), ())), preferred_element_type=jnp.float32
            )
            return raw * factor + (line_gate - gate_row[j])

        def weigh(weights, j):
            return jnp.dot(
                weights.astype(jnp.bfloat16), v_buf[j], preferred_element_type=jnp.float32
            )

        scores = jnp.where(causal, scores_of(i), -jnp.inf)
        top = jnp.max(scores, axis=1, keepdims=True)
        weights = jnp.exp2(scores - top)
        total = jnp.sum(weights, axis=1, keepdims=True)
        held = weigh(weights, i)

        def fold(j, state):
            top, total, held = state
            scores = scores_of(j)
            newest = jnp.maximum(top, jnp.max(scores, axis=1, keepdims=True))
            shrink = jnp.exp2(top - newest)
            weights = jnp.exp2(scores - newest)
            total = total * shrink + jnp.sum(weights, axis=1, keepdims=True)
            held = held * shrink + weigh(weights, j)
            return newest, total, held

        top, total, held = lax.fori_loop(0, i, fold, (top, total, held))
        o_buf[i] = (held / total).astype(o_buf.dtype)

        @pl.when(i != me)
        def _():
            back_copy(i).start()

        source = (me + n - i) % n
        spot = routed_ref.at[source, my_tp]
        pltpu.make_async_copy(spot, spot, recv_a.at[source]).wait()

        @pl.loop(1, tp)
        def _(step):
            spread_copy(source, (my_tp + step) % tp).start()

    own = pltpu.make_async_copy(o_buf.at[me], out_ref.at[own_part, own_cols], recv_o.at[me])
    own.start()

    @pl.loop(1, heads)
    def _(step):
        head = (my_head + step) % heads
        k_copy(head * members + my_member, head).wait_send()
        v_copy(head * members + my_member, head).wait_send()

    @pl.loop(1, n)
    def _(step):
        q_copy((me + step) % n).wait_send()
        back_copy((me + step) % n).wait_send()
        leave_copy((me + step) % n).wait_send()

    @pl.loop(1, tp)
    def _(step):
        token_copy((my_tp + step) % tp).wait_send()

    @pl.loop(0, n)
    def _(source):
        @pl.loop(1, tp)
        def _(step):
            other = (my_tp + step) % tp
            spread_copy(source, other).wait_send()
            spot = routed_ref.at[source, other]
            pltpu.make_async_copy(spot, spot, recv_f.at[source, other]).wait()

    @pl.loop(0, heads)
    def _(step):
        source = step * members + my_member

        @pl.loop(1, members)
        def _(other):
            for copy in pass_copies(source, my_head * members + (my_member + other) % members):
                copy.wait_send()

    @pl.loop(0, n)
    def _(i):
        cols = pl.ds(pl.multiple_of((i // members) * width, width), width)
        part = pl.ds(pl.multiple_of((i % members) * chunk, chunk), chunk)
        spot = out_ref.at[part, cols]
        pltpu.make_async_copy(spot, spot, recv_o.at[i]).wait()


def attention(queries, key_rows, values, forget_log, picks, normed):
    n, tp = lax.axis_size("ep"), lax.axis_size("tp")
    share, depth = picks.shape[1], normed.shape[1]
    rows, heads = queries.shape[0], forget_log.shape[1]
    width = queries.shape[1] // heads
    members = n // heads
    chunk = rows // members
    me = lax.axis_index("ep")
    gates = lax.dynamic_slice_in_dim(forget_log.T * LOG2E, me // members, 1, 0)
    gate_row = gates.reshape(n, 1, rows)
    gate_col = lax.dynamic_slice_in_dim(
        gates.reshape(n, members, chunk), me % members, 1, 1
    ).reshape(n, chunk, 1)
    vmem = pl.BlockSpec(memory_space=pltpu.VMEM)
    dma = pltpu.SemaphoreType.DMA
    blocks = n * (n + 1) // 2
    return pl.pallas_call(
        functools.partial(attention_kernel, n, tp, heads),
        out_shape=(
            jax.ShapeDtypeStruct((rows, heads * width), jnp.bfloat16),
            jax.ShapeDtypeStruct((n, tp, share, depth), jnp.bfloat16),
        ),
        in_specs=[vmem] * 7,
        out_specs=(vmem, vmem),
        scratch_shapes=[
            pltpu.VMEM((n, rows, width), jnp.bfloat16),
            pltpu.VMEM((n, rows, width), jnp.bfloat16),
            pltpu.VMEM((n, chunk, width), jnp.bfloat16),
            pltpu.VMEM((n, chunk, width), jnp.bfloat16),
            pltpu.VMEM((tp * normed.shape[0], depth), jnp.bfloat16),
            pltpu.VMEM((n, share, depth), jnp.bfloat16),
            dma((n,)), dma((n,)), dma((n,)), dma((n,)),
            dma((heads,)), dma((heads,)), dma((n,)), dma((n,)),
            dma((n, members)), dma((n, members)),
            dma((tp,)), dma((tp,)), dma((n,)), dma((n,)), dma((n, tp)), dma((n, tp)),
        ],
        compiler_params=pltpu.CompilerParams(
            collective_id=0, has_side_effects=True, vmem_limit_bytes=40 * 1024 * 1024
        ),
        cost_estimate=pl.CostEstimate(
            flops=40 * blocks * chunk * rows * width, bytes_accessed=8 * rows * heads * width,
            transcendentals=blocks * chunk * rows,
        ),
    )(gate_row, gate_col, queries, key_rows, values, picks, normed)


def slot_places(route_rows, experts, capacity):
    entries = route_rows.reshape(-1)
    matches = (entries[:, None] == jnp.arange(experts, dtype=jnp.int32)[None, :]).astype(jnp.int32)
    earlier = jnp.cumsum(matches, axis=0) - matches
    ranking = jnp.sum(earlier * matches, axis=1)
    return entries * capacity + ranking


def staged(
    queries,
    key_rows,
    values,
    forget_log,
    out_weight,
    expert_input,
    norm_gain,
    route_ids,
    route_weights,
    gate_weight,
    up_weight,
    down_weight,
):
    as_float = expert_input.astype(jnp.float32)
    center = jnp.mean(as_float, axis=1, keepdims=True)
    variance = jnp.mean(jnp.square(as_float - center), axis=1, keepdims=True)
    normed = ((as_float - center) * lax.rsqrt(variance + EPSILON) * norm_gain).astype(jnp.bfloat16)
    block_rows = route_ids.shape[0]
    chosen = route_ids.shape[1]
    expert_local = gate_weight.shape[0]
    ep_count = lax.axis_size("ep")
    tp_count = lax.axis_size("tp")
    experts = expert_local * ep_count
    capacity = block_rows * chosen * 2 // experts
    places = slot_places(route_ids, experts, capacity)
    share_size = capacity // tp_count
    own_slots = lax.axis_index("tp") * share_size + jnp.arange(share_size, dtype=jnp.int32)
    part_slots = jnp.arange(experts, dtype=jnp.int32)[:, None] * capacity + own_slots[None, :]
    picks = jnp.any(
        part_slots.reshape(ep_count, expert_local * share_size)[:, :, None, None]
        == places.reshape(block_rows, chosen).T[None, None, :, :],
        axis=2,
    ).astype(jnp.bfloat16)
    attended, routed = attention(queries, key_rows, values, forget_log, picks, normed)
    arrived_rows = (
        routed.reshape(ep_count, tp_count, expert_local, share_size, routed.shape[3])
        .transpose(0, 2, 1, 3, 4)
        .reshape(ep_count, expert_local, capacity, routed.shape[3])
    )
    gate_part = jnp.einsum(
        "sxcd,xdf->sxcf", arrived_rows, gate_weight, preferred_element_type=jnp.float32
    )
    up_part = jnp.einsum(
        "sxcd,xdf->sxcf", arrived_rows, up_weight, preferred_element_type=jnp.float32
    )
    hidden = (jax.nn.silu(gate_part) * up_part).astype(jnp.bfloat16)
    slots_all = ep_count * expert_local * capacity
    flat_hidden = hidden.reshape(slots_all, hidden.shape[3])
    out_width = out_weight.shape[1]
    mixer_sum = jnp.dot(
        lax.all_gather(attended, "tp", axis=1, tiled=True),
        out_weight,
        preferred_element_type=jnp.float32,
    )
    part_rows = lax.all_gather(flat_hidden, "tp", axis=1, tiled=True)
    shaped = part_rows.reshape(ep_count, expert_local, capacity, part_rows.shape[1])
    product = jnp.einsum("sxcf,xfd->sxcd", shaped, down_weight, preferred_element_type=jnp.float32)
    expert_sum = product.reshape(slots_all, out_width)
    leaving = expert_sum.astype(jnp.bfloat16).reshape(ep_count, expert_local, capacity, out_width)
    returned = lax.all_to_all(leaving, "ep", split_axis=0, concat_axis=0, tiled=True)
    picked = jnp.take(returned.reshape(experts * capacity, out_width), places, axis=0).astype(
        jnp.float32
    )
    combined = jnp.sum(
        (picked * route_weights.reshape(-1)[:, None]).reshape(block_rows, chosen, out_width), axis=1
    )
    return (mixer_sum.astype(jnp.bfloat16), combined.astype(jnp.bfloat16))


def fused_kernel(
    n, tp, heads, cores, q_ref, k_ref, v_ref, gate_ref, x_ref, gain_ref, ids_ref, mix_ref,
    wg_ref, wu_ref, wd_ref, wo_ref,
    mixed_ref, expert_ref,
    wg, wu, wd, wo, x_buf, token_buf, leave_buf, routed, hidden, product, back, comb_hi, comb_lo,
    k_buf, v_buf, q_buf, o_buf, own_buf, own_lse, part_buf, part_lse, got_buf, got_lse, attended,
    load, send_k, recv_k, send_v, recv_v, send_q, recv_q, send_o, recv_o,
    send_p, recv_p, send_l, recv_l, send_t, recv_t, send_a, recv_a, send_f, recv_f,
    send_h, recv_h, send_r, recv_r, send_m, recv_m,
):
    groups = n // heads
    chips = tp // cores
    rows = k_ref.shape[0]
    width = k_ref.shape[1] // heads
    halves = q_buf.shape[1]
    chunk = rows // halves
    tokens, depth = x_ref.shape
    share = leave_buf.shape[0] // n
    capacity = share * tp
    block_rows = token_buf.shape[0]
    chosen = ids_ref.shape[0]
    inner = wg.shape[1]
    out_width = wo.shape[1]
    factor = LOG2E * width ** (-0.5)
    me, my_tp = lax.axis_index("ep"), lax.axis_index("tp")
    my_group, my_head = me // heads, me % heads
    my_chip, my_core = my_tp // cores, my_tp % cores
    base = my_group * heads

    siblings = [my_chip * cores + (my_core + s) % cores for s in range(1, cores)]
    across = [((my_chip + s) % chips) * cores + my_core for s in range(1, chips)]
    rest = [
        ((my_chip + s) % chips) * cores + (my_core + r) % cores
        for s in range(1, chips) for r in range(1, cores)
    ]

    def span(start, size):
        return pl.ds(pl.multiple_of(start * size, size), size)

    def arrived(ref, sem):
        pltpu.make_async_copy(ref, ref, sem).wait()

    def to_ep(src, dst, send, recv, target):
        return pltpu.make_async_remote_copy(
            src_ref=src, dst_ref=dst, send_sem=send, recv_sem=recv, device_id={"ep": target}
        )

    def gather(piece, sends, recvs, first):
        def copy(owner, target):
            return pltpu.make_async_remote_copy(
                src_ref=piece(owner), dst_ref=piece(owner), send_sem=sends.at[first + owner, target],
                recv_sem=recvs.at[first + owner], device_id={"tp": target},
            )

        def start():
            for target in across + siblings:
                copy(my_tp, target).start()

        def forward():
            for owner in across:
                arrived(piece(owner), recvs.at[first + owner])
                for target in siblings:
                    copy(owner, target).start()

        def finish():
            for owner in siblings + rest:
                arrived(piece(owner), recvs.at[first + owner])

        def drain():
            for target in across + siblings:
                copy(my_tp, target).wait_send()
            for owner in across:
                for target in siblings:
                    copy(owner, target).wait_send()

        return start, forward, finish, drain

    def token_piece(owner):
        return token_buf.at[span(owner, tokens), :]

    def routed_piece(source):
        return lambda owner: routed.at[span(source * tp + owner, share), :]

    parts = send_h.shape[0] // tp
    strip = inner // parts

    def hidden_piece(part):
        return lambda owner: hidden.at[:, span(owner * parts + part, strip)]

    def mixed_piece(head):
        return lambda owner: attended.at[:, span(owner * heads + head, width)]

    token_gather = gather(token_piece, send_t, recv_t, 0)

    def spread(source):
        return gather(routed_piece(source), send_f, recv_f, source * tp)

    def hidden_gather(part):
        return gather(hidden_piece(part), send_h, recv_h, part * tp)

    def mixed_gather(head):
        return gather(mixed_piece(head), send_m, recv_m, head * tp)

    loads = [
        pltpu.make_async_copy(src, dst, load.at[i])
        for i, (src, dst) in enumerate((
            (x_ref, x_buf), (wg_ref.at[0], wg), (wu_ref.at[0], wu), (wd_ref.at[0], wd), (wo_ref, wo),
        ))
    ]
    loads[0].start()

    barrier = pltpu.get_barrier_semaphore()

    @pl.loop(1, n)
    def _(step):
        pl.semaphore_signal(barrier, inc=1, device_id={"ep": (me + step) % n})

    @pl.loop(1, tp)
    def _(step):
        pl.semaphore_signal(barrier, inc=1, device_id={"tp": (my_tp + step) % tp})

    loads[0].wait()
    as_float = x_buf[...].astype(jnp.float32)
    center = jnp.mean(as_float, axis=1, keepdims=True)
    shifted = as_float - center
    variance = jnp.mean(jnp.square(shifted), axis=1, keepdims=True)
    token_buf[span(my_tp, tokens), :] = (
        shifted * lax.rsqrt(variance + EPSILON) * gain_ref[...]
    ).astype(token_buf.dtype)

    pl.semaphore_wait(barrier, n + tp - 2)
    token_gather[0]()

    def kv_copies(head):
        cols = span(head, width)
        target = base + head
        return (
            to_ep(k_ref.at[:, cols], k_buf.at[my_head], send_k.at[head], recv_k.at[my_head], target),
            to_ep(v_ref.at[:, cols], v_buf.at[my_head], send_v.at[head], recv_v.at[my_head], target),
        )

    def q_copy(group, head, half):
        target = group * heads + head
        return to_ep(
            q_ref.at[span(half, chunk), span(head, width)], q_buf.at[me, half],
            send_q.at[target, half], recv_q.at[me, half], target,
        )

    own_cols = span(my_head, width)
    keep_k = pltpu.make_async_copy(k_ref.at[:, own_cols], k_buf.at[my_head], recv_k.at[my_head])
    keep_v = pltpu.make_async_copy(v_ref.at[:, own_cols], v_buf.at[my_head], recv_v.at[my_head])
    keep_k.start()
    keep_v.start()
    for half in range(halves):
        pltpu.make_async_copy(
            q_ref.at[span(half, chunk), own_cols], q_buf.at[me, half], recv_q.at[me, half]
        ).start()

    def lower_queries(half):
        @pl.loop(0, my_group)
        def _(group):
            @pl.loop(0, heads)
            def _(step):
                q_copy(group, (my_head + step) % heads, half).start()

    @pl.loop(1, heads)
    def _(step):
        for copy in kv_copies((my_head + step) % heads):
            copy.start()

    lower_queries(0)

    @pl.loop(1, heads)
    def _(step):
        for half in range(halves):
            q_copy(my_group, (my_head + step) % heads, half).start()

    for copy in loads[1:]:
        copy.start()

    expert = lax.broadcasted_iota(jnp.int32, (n, block_rows), 0)
    named = jnp.zeros((n, block_rows), jnp.float32)
    scale = jnp.zeros((n, block_rows), jnp.float32)
    for k in range(chosen):
        match = expert == ids_ref[k : k + 1, :]
        named = jnp.where(match, 1.0, named)
        scale = jnp.where(match, mix_ref[k : k + 1, :], scale)
    before = lax.broadcasted_iota(jnp.int32, (block_rows, block_rows), 0)
    after = lax.broadcasted_iota(jnp.int32, (block_rows, block_rows), 1)
    ranks = jnp.dot(
        named.astype(jnp.bfloat16), jnp.where(before < after, 1.0, 0.0).astype(jnp.bfloat16),
        preferred_element_type=jnp.float32,
    )

    def per_slot(table, count):
        return jnp.broadcast_to(table[:, None, :], (n, count, block_rows))

    slots = lax.broadcasted_iota(jnp.int32, (n, share, block_rows), 1) + my_tp * share
    picks = jnp.where(
        per_slot(ranks, share) == slots.astype(jnp.float32), per_slot(named, share), 0.0
    ).reshape(n * share, block_rows).astype(jnp.bfloat16)

    token_gather[1]()
    token_gather[2]()

    piece = depth // 8

    @pl.loop(0, depth // piece)
    def _(i):
        cols = span(i, piece)
        leave_buf[:, cols] = jnp.dot(
            picks, token_buf[:, cols], preferred_element_type=jnp.float32
        ).astype(leave_buf.dtype)

    def leave_copy(target):
        return to_ep(
            leave_buf.at[span(target, share), :], routed_piece(me)(my_tp),
            send_a.at[target], recv_a.at[me], target,
        )

    pltpu.make_async_copy(
        leave_buf.at[span(me, share), :], routed_piece(me)(my_tp), recv_a.at[me]
    ).start()

    @pl.loop(1, n)
    def _(step):
        leave_copy((me + step) % n).start()

    lower_queries(1)

    all_slots = lax.broadcasted_iota(jnp.int32, (n, capacity, block_rows), 1)
    comb = jnp.where(
        per_slot(ranks, capacity) == all_slots.astype(jnp.float32), per_slot(scale, capacity), 0.0
    ).reshape(n * capacity, block_rows)
    comb = jnp.where(
        jnp.broadcast_to(named[:, None, :], (n, capacity, block_rows)).reshape(
            n * capacity, block_rows) > 0.0, comb, 0.0
    ).T
    high = comb.astype(jnp.bfloat16)
    comb_hi[...] = high
    comb_lo[...] = (comb - high.astype(jnp.float32)).astype(jnp.bfloat16)

    @pl.loop(0, heads)
    def _(step):
        source = (my_head + step) % heads
        arrived(k_buf.at[source], recv_k.at[source])
        arrived(v_buf.at[source], recv_v.at[source])

    def key_gate(source):
        return gate_ref[pl.ds(my_head, 1), span(base + source, rows)] * LOG2E

    def line_gate(i, half):
        line = gate_ref[pl.ds(my_head, 1), span(i * halves + half, chunk)] * LOG2E
        return jnp.broadcast_to(line, (width, chunk)).T[:, :1]

    def attend(i, half, first, count, causal):
        query = q_buf[i, half]
        gate = line_gate(i, half)

        def scores_of(source):
            raw = lax.dot_general(
                query, k_buf[source], (((1,), (1,)), ((), ())), preferred_element_type=jnp.float32
            )
            return raw * factor - key_gate(source)

        def weigh(weights, source):
            return jnp.dot(
                weights.astype(jnp.bfloat16), v_buf[source], preferred_element_type=jnp.float32
            )

        scores = scores_of(first)
        if causal:
            column = lax.broadcasted_iota(jnp.int32, (chunk, rows), 1)
            line = lax.broadcasted_iota(jnp.int32, (chunk, rows), 0) + half * chunk
            scores = jnp.where(column <= line, scores, -jnp.inf)
        top = jnp.max(scores, axis=1, keepdims=True) + gate
        weights = jnp.exp2(scores - (top - gate))
        total = jnp.sum(weights, axis=1, keepdims=True)
        held = weigh(weights, first)

        def fold(source, state):
            top, total, held = state
            scores = scores_of(source)
            newest = jnp.maximum(top, jnp.max(scores, axis=1, keepdims=True) + gate)
            shrink = jnp.exp2(top - newest)
            weights = jnp.exp2(scores - (newest - gate))
            total = total * shrink + jnp.sum(weights, axis=1, keepdims=True)
            held = held * shrink + weigh(weights, source)
            return newest, total, held

        top, total, held = lax.fori_loop(0, count, fold, (top, total, held))
        return held / total, top + jnp.log(total) * LOG2E

    def back_copy(source, half):
        return to_ep(
            o_buf.at[source, half], attended.at[span(half, chunk), span(my_tp * heads + my_head, width)],
            send_o.at[source, half], recv_o.at[my_head, half], base + source,
        )

    def give(source, half):
        @pl.when(source != my_head)
        def _():
            back_copy(source, half).start()

        @pl.when(source == my_head)
        def _():
            pltpu.make_async_copy(
                o_buf.at[source, half],
                attended.at[span(half, chunk), span(my_tp * heads + my_head, width)],
                recv_o.at[my_head, half],
            ).start()

    def spread_step(step):
        source = (me + n - step) % n
        arrived(routed_piece(source)(my_tp), recv_a.at[source])
        spread(source)[0]()

    per_head = n // heads

    @pl.loop(0, heads)
    def _(source):
        for half in range(halves):
            i = base + source
            arrived(q_buf.at[i, half], recv_q.at[i, half])
            out, lse = attend(i, half, source, source, True)

            @pl.when(my_group == 0)
            def _():
                o_buf[source, half] = out.astype(o_buf.dtype)
                give(source, half)

            @pl.when(my_group > 0)
            def _():
                own_buf[source, half] = out
                own_lse[source, half] = jnp.broadcast_to(lse, (chunk, width))

        for s in range(per_head):
            spread_step(source * per_head + s)

    def part_copies(i, half):
        slot = i % heads
        return (
            to_ep(part_buf.at[i, half], got_buf.at[my_group, slot, half],
                  send_p.at[i, half], recv_p.at[my_group, slot * halves + half],
                  (i // heads) * heads + my_head),
            to_ep(part_lse.at[i, half], got_lse.at[my_group, slot, half],
                  send_l.at[i, half], recv_l.at[my_group, slot * halves + half],
                  (i // heads) * heads + my_head),
        )

    def later_queries(half):
        @pl.loop(base + heads, n)
        def _(i):
            arrived(q_buf.at[i, half], recv_q.at[i, half])
            out, lse = attend(i, half, heads - 1, heads - 1, False)
            part_buf[i, half] = out.astype(part_buf.dtype)
            part_lse[i, half] = jnp.broadcast_to(lse, (chunk, width)).T[: part_lse.shape[2], :]
            for copy in part_copies(i, half):
                copy.start()

    later_queries(0)

    @pl.loop(0, n)
    def _(step):
        spread((me + n - step) % n)[1]()

    @pl.loop(0, n)
    def _(step):
        spread((me + n - step) % n)[2]()

    loads[1].wait()
    loads[2].wait()
    for part in range(parts):
        cols = slice(part * strip, (part + 1) * strip)
        gate_part = jnp.dot(routed[...], wg[:, cols], preferred_element_type=jnp.float32)
        up_part = jnp.dot(routed[...], wu[:, cols], preferred_element_type=jnp.float32)
        hidden[:, span(my_tp * parts + part, strip)] = (
            gate_part / (1.0 + jnp.exp(-gate_part)) * up_part
        ).astype(hidden.dtype)
        hidden_gather(part)[0]()

    later_queries(1)

    for part in range(parts):
        hidden_gather(part)[1]()

    def merge(half):
        @pl.when(my_group > 0)
        def _():
            @pl.loop(0, heads)
            def _(source):
                @pl.loop(0, my_group)
                def _(group):
                    place = source * halves + half
                    arrived(got_buf.at[group, source, half], recv_p.at[group, place])
                    arrived(got_lse.at[group, source, half], recv_l.at[group, place])
                    line = got_lse[group, source, half][:1, :]
                    theirs = jnp.broadcast_to(line, (width, chunk)).T
                    mine = own_lse[source, half]
                    top = jnp.maximum(mine, theirs)
                    a, b = jnp.exp2(mine - top), jnp.exp2(theirs - top)
                    total = a + b
                    own_buf[source, half] = (
                        own_buf[source, half] * a
                        + got_buf[group, source, half].astype(jnp.float32) * b
                    ) / total
                    own_lse[source, half] = top + jnp.log(total) * LOG2E

                o_buf[source, half] = own_buf[source, half].astype(o_buf.dtype)
                give(source, half)

    merge(0)

    for part in range(parts):
        hidden_gather(part)[2]()
    loads[3].wait()
    tiles = 2
    tall = n * capacity // tiles
    each = n // tiles

    def return_copy(target):
        return to_ep(
            product.at[span(target, capacity), :], back.at[span(me, capacity), :],
            send_r.at[target], recv_r.at[me], target,
        )

    @pl.loop(0, tiles)
    def _(step):
        tile = (step + 1 + me // each) % tiles
        lines = span(tile, tall)
        product[lines, :] = jnp.dot(
            hidden[lines, :], wd[...], preferred_element_type=jnp.float32
        ).astype(product.dtype)

        @pl.loop(0, each)
        def _(place):
            target = tile * each + (place + me) % each

            @pl.when(target != me)
            def _():
                return_copy(target).start()

            @pl.when(target == me)
            def _():
                pltpu.make_async_copy(
                    product.at[span(me, capacity), :], back.at[span(me, capacity), :], recv_r.at[me]
                ).start()

    for half in range(1, halves):
        merge(half)

    @pl.loop(0, heads)
    def _(step):
        head = (my_head + step) % heads
        for half in range(halves):
            arrived(
                attended.at[span(half, chunk), span(my_tp * heads + head, width)],
                recv_o.at[head, half],
            )
        mixed_gather(head)[0]()

    @pl.loop(0, heads)
    def _(step):
        mixed_gather((my_head + step) % heads)[1]()

    @pl.loop(0, heads)
    def _(head):
        mixed_gather(head)[2]()

    loads[4].wait()

    @pl.loop(0, 2)
    def _(step):
        lines = span(step, rows // 2)
        mixed_ref[lines, :] = jnp.dot(
            attended[lines, :], wo[...], preferred_element_type=jnp.float32
        ).astype(mixed_ref.dtype)

    @pl.loop(0, n)
    def _(source):
        arrived(back.at[span(source, capacity), :], recv_r.at[source])

    expert_ref[...] = (
        jnp.dot(comb_hi[...], back[...], preferred_element_type=jnp.float32)
        + jnp.dot(comb_lo[...], back[...], preferred_element_type=jnp.float32)
    ).astype(expert_ref.dtype)

    token_gather[3]()

    @pl.loop(1, heads)
    def _(step):
        head = (my_head + step) % heads
        for copy in kv_copies(head):
            copy.wait_send()
        for half in range(halves):
            q_copy(my_group, head, half).wait_send()
            back_copy(head, half).wait_send()

    @pl.loop(0, my_group)
    def _(group):
        @pl.loop(0, heads)
        def _(head):
            for half in range(halves):
                q_copy(group, head, half).wait_send()

    @pl.loop(base + heads, n)
    def _(i):
        for half in range(halves):
            for copy in part_copies(i, half):
                copy.wait_send()

    @pl.loop(1, n)
    def _(step):
        leave_copy((me + step) % n).wait_send()
        return_copy((me + step) % n).wait_send()

    @pl.loop(0, n)
    def _(source):
        spread(source)[3]()

    for part in range(parts):
        hidden_gather(part)[3]()

    @pl.loop(0, heads)
    def _(head):
        mixed_gather(head)[3]()


def fused(
    cores, queries, key_rows, values, forget_log, out_weight, expert_input, norm_gain, route_ids,
    route_weights, gate_weight, up_weight, down_weight,
):
    n, tp = lax.axis_size("ep"), lax.axis_size("tp")
    rows, heads = queries.shape[0], forget_log.shape[1]
    width = queries.shape[1] // heads
    groups, halves, parts = n // heads, 2, 2
    chunk = rows // halves
    tokens, depth = expert_input.shape
    block_rows, chosen = route_ids.shape
    capacity = block_rows * chosen * 2 // n
    share = capacity // tp
    slots = n * capacity
    inner, out_width = gate_weight.shape[2], out_weight.shape[1]
    half_type, wide = jnp.bfloat16, jnp.float32
    vmem, hbm = pl.BlockSpec(memory_space=pltpu.VMEM), pl.BlockSpec(memory_space=pl.ANY)
    dma = pltpu.SemaphoreType.DMA
    blocks = n * n // 2
    return pl.pallas_call(
        functools.partial(fused_kernel, n, tp, heads, cores),
        out_shape=(
            jax.ShapeDtypeStruct((rows, out_width), half_type),
            jax.ShapeDtypeStruct((block_rows, out_width), half_type),
        ),
        in_specs=[hbm, hbm, hbm, vmem, hbm, vmem, vmem, vmem, hbm, hbm, hbm, hbm],
        out_specs=(vmem, vmem),
        scratch_shapes=[
            pltpu.VMEM((depth, inner), half_type), pltpu.VMEM((depth, inner), half_type),
            pltpu.VMEM((inner * tp, out_width), half_type),
            pltpu.VMEM((width * heads * tp, out_width), half_type),
            pltpu.VMEM((tokens, depth), half_type), pltpu.VMEM((block_rows, depth), half_type),
            pltpu.VMEM((n * share, depth), half_type), pltpu.VMEM((slots, depth), half_type),
            pltpu.VMEM((slots, inner * tp), half_type), pltpu.VMEM((slots, out_width), half_type),
            pltpu.VMEM((slots, out_width), half_type),
            pltpu.VMEM((block_rows, slots), half_type), pltpu.VMEM((block_rows, slots), half_type),
            pltpu.VMEM((heads, rows, width), half_type), pltpu.VMEM((heads, rows, width), half_type),
            pltpu.VMEM((n, halves, chunk, width), half_type),
            pltpu.VMEM((heads, halves, chunk, width), half_type),
            pltpu.VMEM((heads, halves, chunk, width), wide),
            pltpu.VMEM((heads, halves, chunk, width), wide),
            pltpu.VMEM((n, halves, chunk, width), half_type),
            pltpu.VMEM((n, halves, 8, chunk), wide),
            pltpu.VMEM((groups, heads, halves, chunk, width), half_type),
            pltpu.VMEM((groups, heads, halves, 8, chunk), wide),
            pltpu.VMEM((rows, width * heads * tp), half_type),
            dma((5,)), dma((heads,)), dma((heads,)), dma((heads,)), dma((heads,)),
            dma((n, halves)), dma((n, halves)), dma((heads, halves)), dma((heads, halves)),
            dma((n, halves)), dma((groups, heads * halves)),
            dma((n, halves)), dma((groups, heads * halves)),
            dma((tp, tp)), dma((tp,)), dma((n,)), dma((n,)), dma((n * tp, tp)), dma((n * tp,)),
            dma((parts * tp, tp)), dma((parts * tp,)), dma((n,)), dma((n,)),
            dma((heads * tp, tp)), dma((heads * tp,)),
        ],
        compiler_params=pltpu.CompilerParams(
            collective_id=0, has_side_effects=True, vmem_limit_bytes=58 * 1024 * 1024
        ),
        cost_estimate=pl.CostEstimate(
            flops=6 * slots * depth * inner + 2 * rows * rows * width * blocks,
            bytes_accessed=8 * depth * inner, transcendentals=blocks * rows * rows,
        ),
    )(
        queries, key_rows, values, forget_log.T, expert_input, norm_gain.reshape(1, depth),
        route_ids.T, route_weights.T, gate_weight, up_weight, down_weight, out_weight,
    )


def chip_cores(mesh):
    names = list(mesh.axis_names)
    line = mesh.devices.transpose(names.index("ep"), names.index("tp"))[0]
    spots = [getattr(device, "coords", i) for i, device in enumerate(line)]
    spots = [tuple(spot) if hasattr(spot, "__len__") else spot for spot in spots]
    cores = sum(spot == spots[0] for spot in spots)
    even = len(spots) % cores == 0 and all(
        spots[i] == spots[i - i % cores] for i in range(len(spots))
    )
    return cores if even else 1


def fits(n, tp, heads, block_rows, chosen, local_experts, inner):
    capacity = block_rows * chosen * 2 // (n * local_experts)
    return (
        local_experts == 1 and n % heads == 0 and heads > 1 and capacity % (16 * tp) == 0
        and n % 2 == 0 and inner % 256 == 0
    )


def choose(cores, *args):
    n, tp = lax.axis_size("ep"), lax.axis_size("tp")
    ids, gate_weight = args[7], args[9]
    if fits(
        n, tp, args[3].shape[1], ids.shape[0], ids.shape[1], gate_weight.shape[0],
        gate_weight.shape[2],
    ):
        return fused(cores, *args)
    return staged(*args)


def solution(mesh):
    placed = (
        P("ep", "tp"),
        P("ep", "tp"),
        P("ep", "tp"),
        P(None, "tp"),
        P(None, "tp"),
        P(("ep", "tp"), None),
        P(),
        P("ep", None),
        P("ep", None),
        P("ep", None, "tp"),
        P("ep", None, "tp"),
        P("ep", None, "tp"),
    )
    return jax.shard_map(
        functools.partial(choose, chip_cores(mesh)), mesh=mesh, in_specs=placed, out_specs=(P("ep", "tp"), P("ep", "tp")), check_vma=False
    )
```

```python
import functools
import math

import jax
import jax.numpy as jnp
from jax import lax
from jax.experimental import pallas as pl
from jax.experimental.pallas import tpu as pltpu
from jax.sharding import PartitionSpec as P

EPSILON = 1e-05
LOG2E = math.log2(math.e)


def attention_kernel(
    n, tp, heads, gate_row, gate_col, q_ref, k_ref, v_ref, pick_ref, token_ref,
    out_ref, routed_ref,
    k_buf, v_buf, q_buf, o_buf, token_buf, leave_buf,
    recv_k, recv_v, recv_q, recv_o, send_k, send_v, send_q, send_o, pass_k, pass_v,
    send_t, recv_t, send_a, recv_a, send_f, recv_f,
):
    members = n // heads
    rows = k_ref.shape[0]
    width = k_ref.shape[1] // heads
    chunk = rows // members
    me = lax.axis_index("ep")
    my_member = me % members
    my_head = me // members
    my_tp = lax.axis_index("tp")
    tokens = token_ref.shape[0]

    barrier = pltpu.get_barrier_semaphore()

    @pl.loop(1, n)
    def _(step):
        pl.semaphore_signal(barrier, inc=1, device_id={"ep": (me + step) % n})

    @pl.loop(1, tp)
    def _(step):
        pl.semaphore_signal(barrier, inc=1, device_id={"tp": (my_tp + step) % tp})

    pl.semaphore_wait(barrier, n + tp - 2)

    def k_copy(target, head):
        cols = pl.ds(pl.multiple_of(head * width, width), width)
        return pltpu.make_async_remote_copy(
            src_ref=k_ref.at[:, cols], dst_ref=k_buf.at[me], send_sem=send_k.at[head],
            recv_sem=recv_k.at[me], device_id={"ep": target},
        )

    def v_copy(target, head):
        cols = pl.ds(pl.multiple_of(head * width, width), width)
        return pltpu.make_async_remote_copy(
            src_ref=v_ref.at[:, cols], dst_ref=v_buf.at[me], send_sem=send_v.at[head],
            recv_sem=recv_v.at[me], device_id={"ep": target},
        )

    def q_copy(target):
        cols = pl.ds(pl.multiple_of((target // members) * width, width), width)
        part = pl.ds(pl.multiple_of((target % members) * chunk, chunk), chunk)
        return pltpu.make_async_remote_copy(
            src_ref=q_ref.at[part, cols], dst_ref=q_buf.at[me], send_sem=send_q.at[target],
            recv_sem=recv_q.at[me], device_id={"ep": target},
        )

    def pass_copies(source, target):
        return (
            pltpu.make_async_remote_copy(
                src_ref=k_buf.at[source], dst_ref=k_buf.at[source],
                send_sem=pass_k.at[source, target % members],
                recv_sem=recv_k.at[source], device_id={"ep": target},
            ),
            pltpu.make_async_remote_copy(
                src_ref=v_buf.at[source], dst_ref=v_buf.at[source],
                send_sem=pass_v.at[source, target % members],
                recv_sem=recv_v.at[source], device_id={"ep": target},
            ),
        )

    def back_copy(source):
        cols = pl.ds(pl.multiple_of(my_head * width, width), width)
        part = pl.ds(pl.multiple_of(my_member * chunk, chunk), chunk)
        return pltpu.make_async_remote_copy(
            src_ref=o_buf.at[source], dst_ref=out_ref.at[part, cols], send_sem=send_o.at[source],
            recv_sem=recv_o.at[me], device_id={"ep": source},
        )

    def token_spot(owner):
        return token_buf.at[pl.ds(pl.multiple_of(owner * tokens, tokens), tokens), :]

    def token_copy(target):
        return pltpu.make_async_remote_copy(
            src_ref=token_ref, dst_ref=token_spot(my_tp), send_sem=send_t.at[target],
            recv_sem=recv_t.at[my_tp], device_id={"tp": target},
        )

    def leave_copy(target):
        return pltpu.make_async_remote_copy(
            src_ref=leave_buf.at[target], dst_ref=routed_ref.at[me, my_tp],
            send_sem=send_a.at[target], recv_sem=recv_a.at[me], device_id={"ep": target},
        )

    def spread_copy(source, target):
        spot = routed_ref.at[source, my_tp]
        return pltpu.make_async_remote_copy(
            src_ref=spot, dst_ref=spot, send_sem=send_f.at[source, target],
            recv_sem=recv_f.at[source, my_tp], device_id={"tp": target},
        )

    pltpu.make_async_copy(token_ref, token_spot(my_tp), recv_t.at[my_tp]).start()

    @pl.loop(1, tp)
    def _(step):
        token_copy((my_tp + step) % tp).start()

    own_cols = pl.ds(pl.multiple_of(my_head * width, width), width)
    own_part = pl.ds(pl.multiple_of(my_member * chunk, chunk), chunk)
    pltpu.make_async_copy(k_ref.at[:, own_cols], k_buf.at[me], recv_k.at[me]).start()
    pltpu.make_async_copy(v_ref.at[:, own_cols], v_buf.at[me], recv_v.at[me]).start()
    pltpu.make_async_copy(q_ref.at[own_part, own_cols], q_buf.at[me], recv_q.at[me]).start()

    @pl.loop(1, heads)
    def _(step):
        head = (my_head + step) % heads
        k_copy(head * members + my_member, head).start()
        v_copy(head * members + my_member, head).start()

    @pl.loop(1, n)
    def _(step):
        q_copy((me + step) % n).start()

    @pl.loop(0, tp)
    def _(owner):
        pltpu.make_async_copy(token_spot(owner), token_spot(owner), recv_t.at[owner]).wait()

    @pl.loop(0, n)
    def _(target):
        leave_buf[target] = jnp.dot(
            pick_ref[target], token_buf[...], preferred_element_type=jnp.float32
        ).astype(leave_buf.dtype)

    pltpu.make_async_copy(leave_buf.at[me], routed_ref.at[me, my_tp], recv_a.at[me]).start()

    @pl.loop(1, n)
    def _(step):
        leave_copy((me + step) % n).start()

    def landed(source):
        pltpu.make_async_copy(k_buf.at[source], k_buf.at[source], recv_k.at[source]).wait()
        pltpu.make_async_copy(v_buf.at[source], v_buf.at[source], recv_v.at[source]).wait()

    @pl.loop(0, heads)
    def _(step):
        source = ((my_head + step) % heads) * members + my_member
        landed(source)

        @pl.loop(1, members)
        def _(other):
            for copy in pass_copies(source, my_head * members + (my_member + other) % members):
                copy.start()

    column = lax.broadcasted_iota(jnp.int32, (chunk, rows), 1)
    line = lax.broadcasted_iota(jnp.int32, (chunk, rows), 0) + my_member * chunk
    causal = column <= line
    factor = LOG2E * width ** (-0.5)

    @pl.loop(0, n)
    def _(i):
        pltpu.make_async_copy(q_buf.at[i], q_buf.at[i], recv_q.at[i]).wait()

        @pl.when(i % members != my_member)
        def _():
            landed(i)

        query = q_buf[i]
        line_gate = gate_col[i]

        def scores_of(j):
            raw = lax.dot_general(
                query, k_buf[j], (((1,), (1,)), ((), ())), preferred_element_type=jnp.float32
            )
            return raw * factor + (line_gate - gate_row[j])

        def weigh(weights, j):
            return jnp.dot(
                weights.astype(jnp.bfloat16), v_buf[j], preferred_element_type=jnp.float32
            )

        scores = jnp.where(causal, scores_of(i), -jnp.inf)
        top = jnp.max(scores, axis=1, keepdims=True)
        weights = jnp.exp2(scores - top)
        total = jnp.sum(weights, axis=1, keepdims=True)
        held = weigh(weights, i)

        def fold(j, state):
            top, total, held = state
            scores = scores_of(j)
            newest = jnp.maximum(top, jnp.max(scores, axis=1, keepdims=True))
            shrink = jnp.exp2(top - newest)
            weights = jnp.exp2(scores - newest)
            total = total * shrink + jnp.sum(weights, axis=1, keepdims=True)
            held = held * shrink + weigh(weights, j)
            return newest, total, held

        top, total, held = lax.fori_loop(0, i, fold, (top, total, held))
        o_buf[i] = (held / total).astype(o_buf.dtype)

        @pl.when(i != me)
        def _():
            back_copy(i).start()

        source = (me + n - i) % n
        spot = routed_ref.at[source, my_tp]
        pltpu.make_async_copy(spot, spot, recv_a.at[source]).wait()

        @pl.loop(1, tp)
        def _(step):
            spread_copy(source, (my_tp + step) % tp).start()

    own = pltpu.make_async_copy(o_buf.at[me], out_ref.at[own_part, own_cols], recv_o.at[me])
    own.start()

    @pl.loop(1, heads)
    def _(step):
        head = (my_head + step) % heads
        k_copy(head * members + my_member, head).wait_send()
        v_copy(head * members + my_member, head).wait_send()

    @pl.loop(1, n)
    def _(step):
        q_copy((me + step) % n).wait_send()
        back_copy((me + step) % n).wait_send()
        leave_copy((me + step) % n).wait_send()

    @pl.loop(1, tp)
    def _(step):
        token_copy((my_tp + step) % tp).wait_send()

    @pl.loop(0, n)
    def _(source):
        @pl.loop(1, tp)
        def _(step):
            other = (my_tp + step) % tp
            spread_copy(source, other).wait_send()
            spot = routed_ref.at[source, other]
            pltpu.make_async_copy(spot, spot, recv_f.at[source, other]).wait()

    @pl.loop(0, heads)
    def _(step):
        source = step * members + my_member

        @pl.loop(1, members)
        def _(other):
            for copy in pass_copies(source, my_head * members + (my_member + other) % members):
                copy.wait_send()

    @pl.loop(0, n)
    def _(i):
        cols = pl.ds(pl.multiple_of((i // members) * width, width), width)
        part = pl.ds(pl.multiple_of((i % members) * chunk, chunk), chunk)
        spot = out_ref.at[part, cols]
        pltpu.make_async_copy(spot, spot, recv_o.at[i]).wait()


def attention(queries, key_rows, values, forget_log, picks, normed):
    n, tp = lax.axis_size("ep"), lax.axis_size("tp")
    share, depth = picks.shape[1], normed.shape[1]
    rows, heads = queries.shape[0], forget_log.shape[1]
    width = queries.shape[1] // heads
    members = n // heads
    chunk = rows // members
    me = lax.axis_index("ep")
    gates = lax.dynamic_slice_in_dim(forget_log.T * LOG2E, me // members, 1, 0)
    gate_row = gates.reshape(n, 1, rows)
    gate_col = lax.dynamic_slice_in_dim(
        gates.reshape(n, members, chunk), me % members, 1, 1
    ).reshape(n, chunk, 1)
    vmem = pl.BlockSpec(memory_space=pltpu.VMEM)
    dma = pltpu.SemaphoreType.DMA
    blocks = n * (n + 1) // 2
    return pl.pallas_call(
        functools.partial(attention_kernel, n, tp, heads),
        out_shape=(
            jax.ShapeDtypeStruct((rows, heads * width), jnp.bfloat16),
            jax.ShapeDtypeStruct((n, tp, share, depth), jnp.bfloat16),
        ),
        in_specs=[vmem] * 7,
        out_specs=(vmem, vmem),
        scratch_shapes=[
            pltpu.VMEM((n, rows, width), jnp.bfloat16),
            pltpu.VMEM((n, rows, width), jnp.bfloat16),
            pltpu.VMEM((n, chunk, width), jnp.bfloat16),
            pltpu.VMEM((n, chunk, width), jnp.bfloat16),
            pltpu.VMEM((tp * normed.shape[0], depth), jnp.bfloat16),
            pltpu.VMEM((n, share, depth), jnp.bfloat16),
            dma((n,)), dma((n,)), dma((n,)), dma((n,)),
            dma((heads,)), dma((heads,)), dma((n,)), dma((n,)),
            dma((n, members)), dma((n, members)),
            dma((tp,)), dma((tp,)), dma((n,)), dma((n,)), dma((n, tp)), dma((n, tp)),
        ],
        compiler_params=pltpu.CompilerParams(
            collective_id=0, has_side_effects=True, vmem_limit_bytes=40 * 1024 * 1024
        ),
        cost_estimate=pl.CostEstimate(
            flops=40 * blocks * chunk * rows * width, bytes_accessed=8 * rows * heads * width,
            transcendentals=blocks * chunk * rows,
        ),
    )(gate_row, gate_col, queries, key_rows, values, picks, normed)


def slot_places(route_rows, experts, capacity):
    entries = route_rows.reshape(-1)
    matches = (entries[:, None] == jnp.arange(experts, dtype=jnp.int32)[None, :]).astype(jnp.int32)
    earlier = jnp.cumsum(matches, axis=0) - matches
    ranking = jnp.sum(earlier * matches, axis=1)
    return entries * capacity + ranking


def staged(
    queries,
    key_rows,
    values,
    forget_log,
    out_weight,
    expert_input,
    norm_gain,
    route_ids,
    route_weights,
    gate_weight,
    up_weight,
    down_weight,
):
    as_float = expert_input.astype(jnp.float32)
    center = jnp.mean(as_float, axis=1, keepdims=True)
    variance = jnp.mean(jnp.square(as_float - center), axis=1, keepdims=True)
    normed = ((as_float - center) * lax.rsqrt(variance + EPSILON) * norm_gain).astype(jnp.bfloat16)
    block_rows = route_ids.shape[0]
    chosen = route_ids.shape[1]
    expert_local = gate_weight.shape[0]
    ep_count = lax.axis_size("ep")
    tp_count = lax.axis_size("tp")
    experts = expert_local * ep_count
    capacity = block_rows * chosen * 2 // experts
    places = slot_places(route_ids, experts, capacity)
    share_size = capacity // tp_count
    own_slots = lax.axis_index("tp") * share_size + jnp.arange(share_size, dtype=jnp.int32)
    part_slots = jnp.arange(experts, dtype=jnp.int32)[:, None] * capacity + own_slots[None, :]
    picks = jnp.any(
        part_slots.reshape(ep_count, expert_local * share_size)[:, :, None, None]
        == places.reshape(block_rows, chosen).T[None, None, :, :],
        axis=2,
    ).astype(jnp.bfloat16)
    attended, routed = attention(queries, key_rows, values, forget_log, picks, normed)
    arrived_rows = (
        routed.reshape(ep_count, tp_count, expert_local, share_size, routed.shape[3])
        .transpose(0, 2, 1, 3, 4)
        .reshape(ep_count, expert_local, capacity, routed.shape[3])
    )
    gate_part = jnp.einsum(
        "sxcd,xdf->sxcf", arrived_rows, gate_weight, preferred_element_type=jnp.float32
    )
    up_part = jnp.einsum(
        "sxcd,xdf->sxcf", arrived_rows, up_weight, preferred_element_type=jnp.float32
    )
    hidden = (jax.nn.silu(gate_part) * up_part).astype(jnp.bfloat16)
    slots_all = ep_count * expert_local * capacity
    flat_hidden = hidden.reshape(slots_all, hidden.shape[3])
    out_width = out_weight.shape[1]
    mixer_sum = jnp.dot(
        lax.all_gather(attended, "tp", axis=1, tiled=True),
        out_weight,
        preferred_element_type=jnp.float32,
    )
    part_rows = lax.all_gather(flat_hidden, "tp", axis=1, tiled=True)
    shaped = part_rows.reshape(ep_count, expert_local, capacity, part_rows.shape[1])
    product = jnp.einsum("sxcf,xfd->sxcd", shaped, down_weight, preferred_element_type=jnp.float32)
    expert_sum = product.reshape(slots_all, out_width)
    leaving = expert_sum.astype(jnp.bfloat16).reshape(ep_count, expert_local, capacity, out_width)
    returned = lax.all_to_all(leaving, "ep", split_axis=0, concat_axis=0, tiled=True)
    picked = jnp.take(returned.reshape(experts * capacity, out_width), places, axis=0).astype(
        jnp.float32
    )
    combined = jnp.sum(
        (picked * route_weights.reshape(-1)[:, None]).reshape(block_rows, chosen, out_width), axis=1
    )
    return (mixer_sum.astype(jnp.bfloat16), combined.astype(jnp.bfloat16))


def fused_kernel(
    n, tp, heads, cores, q_ref, k_ref, v_ref, gate_ref, x_ref, gain_ref, ids_ref, mix_ref,
    wg_ref, wu_ref, wd_ref, wo_ref,
    mixed_ref, expert_ref,
    wg, wu, wd, wo, x_buf, token_buf, leave_buf, routed, hidden, product, back, comb_hi, comb_lo,
    ids_buf, mix_buf, sums_out, sums_in,
    k_buf, v_buf, q_buf, o_buf, own_buf, own_lse, part_buf, part_lse, got_buf, got_lse, attended,
    load, send_k, recv_k, send_v, recv_v, send_q, recv_q, send_o, recv_o,
    send_p, recv_p, send_l, recv_l, send_t, recv_t, send_a, recv_a, send_f, recv_f,
    send_h, recv_h, send_r, recv_r, send_m, recv_m,
    send_i, recv_i, send_w, recv_w, send_c, recv_c,
):
    groups = n // heads
    chips = tp // cores
    rows = k_ref.shape[0]
    width = k_ref.shape[1] // heads
    halves = q_buf.shape[1]
    chunk = rows // halves
    tokens, depth = x_ref.shape
    share = leave_buf.shape[0] // n
    capacity = share * tp
    block_rows = token_buf.shape[0]
    chosen = ids_ref.shape[0]
    inner = wg.shape[1]
    out_width = wo.shape[1]
    factor = LOG2E * width ** (-0.5)
    me, my_tp = lax.axis_index("ep"), lax.axis_index("tp")
    my_group, my_head = me // heads, me % heads
    my_chip, my_core = my_tp // cores, my_tp % cores
    base = my_group * heads

    siblings = [my_chip * cores + (my_core + s) % cores for s in range(1, cores)]
    across = [((my_chip + s) % chips) * cores + my_core for s in range(1, chips)]
    rest = [
        ((my_chip + s) % chips) * cores + (my_core + r) % cores
        for s in range(1, chips) for r in range(1, cores)
    ]

    def span(start, size):
        return pl.ds(pl.multiple_of(start * size, size), size)

    def arrived(ref, sem):
        pltpu.make_async_copy(ref, ref, sem).wait()

    def to_ep(src, dst, send, recv, target):
        return pltpu.make_async_remote_copy(
            src_ref=src, dst_ref=dst, send_sem=send, recv_sem=recv, device_id={"ep": target}
        )

    def gather(piece, sends, recvs, first):
        def copy(owner, target):
            return pltpu.make_async_remote_copy(
                src_ref=piece(owner), dst_ref=piece(owner), send_sem=sends.at[first + owner, target],
                recv_sem=recvs.at[first + owner], device_id={"tp": target},
            )

        def start():
            for target in across + siblings:
                copy(my_tp, target).start()

        def forward():
            for owner in across:
                arrived(piece(owner), recvs.at[first + owner])
                for target in siblings:
                    copy(owner, target).start()

        def finish():
            for owner in siblings + rest:
                arrived(piece(owner), recvs.at[first + owner])

        def drain():
            for target in across + siblings:
                copy(my_tp, target).wait_send()
            for owner in across:
                for target in siblings:
                    copy(owner, target).wait_send()

        return start, forward, finish, drain

    def token_piece(owner):
        return token_buf.at[span(owner, tokens), :]

    def routed_piece(source):
        return lambda owner: routed.at[span(source * tp + owner, share), :]

    parts = send_h.shape[0] // tp
    strip = inner // parts

    def hidden_piece(part):
        return lambda owner: hidden.at[:, span(owner * parts + part, strip)]

    def mixed_piece(half):
        return lambda owner: attended.at[span(half, chunk), span(owner, heads * width)]

    token_gather = gather(token_piece, send_t, recv_t, 0)

    def spread(source):
        return gather(routed_piece(source), send_f, recv_f, source * tp)

    def hidden_gather(part):
        return gather(hidden_piece(part), send_h, recv_h, part * tp)

    def mixed_gather(half):
        return gather(mixed_piece(half), send_m, recv_m, half * tp)

    across_groups = [(g, (heads // 2 + s) % heads) for g in range(1, groups) for s in range(heads)]
    in_group = [(0, s) for s in range(1, heads)]
    order = [(0, 0)]
    for place in range(max(len(across_groups), len(in_group))):
        order += across_groups[place : place + 1] + in_group[place : place + 1]

    def peer(step, sign):
        group, head = order[step]
        return ((my_group + groups + sign * group) % groups) * heads + (
            my_head + heads + sign * head
        ) % heads

    loads = [
        pltpu.make_async_copy(src, dst, load.at[i])
        for i, (src, dst) in enumerate((
            (x_ref, x_buf), (wg_ref.at[0], wg), (wu_ref.at[0], wu), (wd_ref.at[0], wd), (wo_ref, wo),
        ))
    ]
    loads[0].start()

    barrier = pltpu.get_barrier_semaphore()

    @pl.loop(1, n)
    def _(step):
        pl.semaphore_signal(barrier, inc=1, device_id={"ep": (me + step) % n})

    @pl.loop(1, tp)
    def _(step):
        pl.semaphore_signal(barrier, inc=1, device_id={"tp": (my_tp + step) % tp})

    loads[0].wait()
    as_float = x_buf[...].astype(jnp.float32)
    center = jnp.mean(as_float, axis=1, keepdims=True)
    shifted = as_float - center
    variance = jnp.mean(jnp.square(shifted), axis=1, keepdims=True)
    token_buf[span(my_tp, tokens), :] = (
        shifted * lax.rsqrt(variance + EPSILON) * gain_ref[...]
    ).astype(token_buf.dtype)

    ids_buf[my_group] = ids_ref[...]
    mix_buf[my_group] = mix_ref[...]
    pl.semaphore_wait(barrier, n + tp - 2)
    token_gather[0]()
    others = [(my_group + step) % groups for step in range(1, groups)]

    def route_copies(group):
        target = group * heads + my_head
        return (
            to_ep(ids_ref, ids_buf.at[my_group], send_i.at[group], recv_i.at[my_group], target),
            to_ep(mix_ref, mix_buf.at[my_group], send_w.at[group], recv_w.at[my_group], target),
        )

    for group in others:
        for copy in route_copies(group):
            copy.start()

    def k_spot(source):
        return k_buf.at[span(source, rows), :width]

    def v_spot(source):
        return v_buf.at[span(source, rows), :width]

    def q_spot(source, half):
        return q_buf.at[source, half, :, :width]

    def kv_copies(head):
        cols = span(head, width)
        target = base + head
        return (
            to_ep(k_ref.at[:, cols], k_spot(my_head), send_k.at[head], recv_k.at[my_head], target),
            to_ep(v_ref.at[:, cols], v_spot(my_head), send_v.at[head], recv_v.at[my_head], target),
        )

    def q_copy(group, head, half):
        target = group * heads + head
        return to_ep(
            q_ref.at[span(half, chunk), span(head, width)], q_spot(me, half),
            send_q.at[target, half], recv_q.at[me, half], target,
        )

    own_cols = span(my_head, width)
    keep_k = pltpu.make_async_copy(k_ref.at[:, own_cols], k_spot(my_head), recv_k.at[my_head])
    keep_v = pltpu.make_async_copy(v_ref.at[:, own_cols], v_spot(my_head), recv_v.at[my_head])
    keep_k.start()
    keep_v.start()
    for half in range(halves):
        pltpu.make_async_copy(
            q_ref.at[span(half, chunk), own_cols], q_spot(me, half), recv_q.at[me, half]
        ).start()

    def lower_queries(half):
        @pl.loop(0, my_group)
        def _(group):
            @pl.loop(0, heads)
            def _(step):
                q_copy(group, (my_head + step) % heads, half).start()

    @pl.loop(1, heads)
    def _(step):
        for copy in kv_copies((my_head + step) % heads):
            copy.start()

    lower_queries(0)

    terms = lax.broadcasted_iota(jnp.int32, (width, chunk), 0)

    def gate_columns(block, sign, offset):
        gate = gate_ref[pl.ds(my_head, 1), span(block, chunk)] * (sign * width**0.5)
        table = jnp.where((terms >= 3 - offset) & (terms < 6 - offset), 1.0, 0.0)
        for place in range(offset, offset + 3):
            piece = gate.astype(jnp.bfloat16).astype(jnp.float32)
            gate = gate - piece
            table = jnp.where(terms == place, piece, table)
        return table.T.astype(jnp.bfloat16)

    v_buf[:, width:] = jnp.ones((heads * rows, width), v_buf.dtype)

    @pl.loop(0, heads * halves)
    def _(place):
        k_buf[span(place, chunk), width:] = gate_columns(base * halves + place, -1.0, 3)

    @pl.loop(base, n)
    def _(i):
        for half in range(halves):
            q_buf[i, half, :, width:] = gate_columns(i * halves + half, 1.0, 0)

    def group_queries(half):
        @pl.loop(1, heads)
        def _(step):
            q_copy(my_group, (my_head + step) % heads, half).start()

    group_queries(0)

    for copy in loads[1:]:
        copy.start()

    before = lax.broadcasted_iota(jnp.int32, (block_rows, block_rows), 0)
    after = lax.broadcasted_iota(jnp.int32, (block_rows, block_rows), 1)
    earlier = jnp.where(before < after, 1.0, 0.0).astype(jnp.bfloat16)

    def places(ids, first, count):
        expert = lax.broadcasted_iota(jnp.int32, (count, block_rows), 0) + first
        matches = [expert == ids[k : k + 1, :] for k in range(chosen)]
        named = functools.reduce(jnp.logical_or, matches)
        ranks = jnp.dot(
            jnp.where(named, 1.0, 0.0).astype(jnp.bfloat16), earlier,
            preferred_element_type=jnp.float32,
        )
        return matches, jnp.where(named, ranks, -1.0)

    def per_slot(table, count):
        return jnp.broadcast_to(table[:, None, :], (table.shape[0], count, block_rows))

    slots = lax.broadcasted_iota(jnp.int32, (n, share, block_rows), 1) + my_tp * share
    picks = jnp.where(
        per_slot(places(ids_ref[...], 0, n)[1], share) == slots.astype(jnp.float32), 1.0, 0.0
    ).reshape(n * share, block_rows).astype(jnp.bfloat16)

    token_gather[1]()
    token_gather[2]()

    piece = depth // 8

    @pl.loop(0, depth // piece)
    def _(i):
        cols = span(i, piece)
        leave_buf[:, cols] = jnp.dot(
            picks, token_buf[:, cols], preferred_element_type=jnp.float32
        ).astype(leave_buf.dtype)

    def leave_copy(target):
        return to_ep(
            leave_buf.at[span(target, share), :], routed_piece(me)(my_tp),
            send_a.at[target], recv_a.at[me], target,
        )

    pltpu.make_async_copy(
        leave_buf.at[span(me, share), :], routed_piece(me)(my_tp), recv_a.at[me]
    ).start()

    for step in range(1, n):
        leave_copy(peer(step, 1)).start()

    for half in range(1, halves):
        group_queries(half)
        lower_queries(half)

    def combining(group):
        matches, ranks = places(ids_buf[group], base, heads)
        scale = functools.reduce(
            jnp.add,
            [
                jnp.where(match, mix_buf[group, k : k + 1, :], 0.0)
                for k, match in enumerate(matches)
            ],
        )
        all_slots = lax.broadcasted_iota(jnp.int32, (heads, capacity, block_rows), 1)
        comb = jnp.where(
            per_slot(ranks, capacity) == all_slots.astype(jnp.float32),
            per_slot(scale, capacity), 0.0,
        ).reshape(heads * capacity, block_rows).T
        high = comb.astype(jnp.bfloat16)
        comb_hi[group] = high
        comb_lo[group] = (comb - high.astype(jnp.float32)).astype(jnp.bfloat16)

    combining(my_group)
    for group in others:
        arrived(ids_buf.at[group], recv_i.at[group])
        arrived(mix_buf.at[group], recv_w.at[group])
        combining(group)

    @pl.loop(0, heads)
    def _(step):
        source = (my_head + step) % heads
        arrived(k_spot(source), recv_k.at[source])
        arrived(v_spot(source), recv_v.at[source])

    stretch = 2 * chunk

    def attend(i, half, keys, causal):
        query = q_buf[i, half]

        def scores_of(lines):
            return lax.dot_general(
                query, k_buf[lines, :], (((1,), (1,)), ((), ())), preferred_element_type=jnp.float32
            )

        open_keys = keys - chunk if causal else keys
        cuts = [
            slice(cut, min(cut + stretch, open_keys)) for cut in range(0, open_keys, stretch)
        ]
        if causal:
            cuts = [slice(open_keys, keys), *cuts]
        scores = scores_of(cuts[0])
        if causal:
            column = lax.broadcasted_iota(jnp.int32, (chunk, chunk), 1)
            line = lax.broadcasted_iota(jnp.int32, (chunk, chunk), 0)
            scores = jnp.where(column <= line, scores, -jnp.inf)
        top = jnp.max(scores, axis=1, keepdims=True)
        held = None
        for place, lines in enumerate(cuts):
            later = scores_of(cuts[place + 1]) if place + 1 < len(cuts) else None
            weights = jnp.exp2((scores - top) * factor).astype(jnp.bfloat16)
            gained = jnp.dot(weights, v_buf[lines, :], preferred_element_type=jnp.float32)
            held = gained if held is None else held + gained
            if later is not None:
                newest = jnp.maximum(top, jnp.max(later, axis=1, keepdims=True))
                held = held * jnp.exp2((top - newest) * factor)
                top, scores = newest, later
        total = held[:, width:]
        return held[:, :width] / total, top * factor + jnp.log(total) * LOG2E

    def back_copy(source, half):
        return to_ep(
            o_buf.at[source, half], attended.at[span(half, chunk), span(my_tp * heads + my_head, width)],
            send_o.at[source, half], recv_o.at[my_head, half], base + source,
        )

    per_head = n // heads

    def give(source, half):
        @pl.when(source != my_head)
        def _():
            back_copy(source, half).start()

        @pl.when(source == my_head)
        def _():
            pltpu.make_async_copy(
                o_buf.at[source, half],
                attended.at[span(half, chunk), span(my_tp * heads + my_head, width)],
                recv_o.at[my_head, half],
            ).start()

    def spread_step(step):
        source = peer(step, -1)
        arrived(routed_piece(source)(my_tp), recv_a.at[source])
        spread(source)[0]()

    def own_queries(source, half):
        i = base + source
        arrived(q_spot(i, half), recv_q.at[i, half])
        out, lse = attend(i, half, source * rows + (half + 1) * chunk, True)

        @pl.when(my_group == 0)
        def _():
            o_buf[source, half] = out.astype(o_buf.dtype)
            give(source, half)

        @pl.when(my_group > 0)
        def _():
            own_buf[source, half] = out
            own_lse[source, half] = lse

    def part_copies(i, half):
        slot = i % heads
        return (
            to_ep(part_buf.at[i, half], got_buf.at[my_group, slot, half],
                  send_p.at[i, half], recv_p.at[my_group, slot * halves + half],
                  (i // heads) * heads + my_head),
            to_ep(part_lse.at[i, half], got_lse.at[my_group, slot, half],
                  send_l.at[i, half], recv_l.at[my_group, slot * halves + half],
                  (i // heads) * heads + my_head),
        )

    def later_queries(group, source, half):
        @pl.when(my_group + group < groups)
        def _():
            i = (my_group + group) * heads + source
            arrived(q_spot(i, half), recv_q.at[i, half])
            out, lse = attend(i, half, heads * rows, False)
            part_buf[i, half] = out.astype(part_buf.dtype)
            part_lse[i, half] = lse.T[: part_lse.shape[2], :]
            for copy in part_copies(i, half):
                copy.start()

    def later_all(half):
        for group in range(1, groups):
            @pl.loop(0, heads)
            def _(source):
                later_queries(group, source, half)

    for step in range(n):
        spread_step(step)
        if step >= 2:
            spread(peer(step - 2, -1))[1]()
        if step < heads:
            own_queries(step, 0)
        elif step < 2 * heads:
            for group in range(1, groups):
                later_queries(group, step - heads, 0)

    for step in range(n - 2, n):
        spread(peer(step, -1))[1]()

    @pl.loop(0, n)
    def _(source):
        spread(source)[2]()

    loads[1].wait()
    loads[2].wait()
    for part in range(parts):
        cols = slice(part * strip, (part + 1) * strip)
        gate_part = jnp.dot(routed[...], wg[:, cols], preferred_element_type=jnp.float32)
        up_part = jnp.dot(routed[...], wu[:, cols], preferred_element_type=jnp.float32)
        hidden[:, span(my_tp * parts + part, strip)] = (
            gate_part / (1.0 + jnp.exp(-gate_part)) * up_part
        ).astype(hidden.dtype)
        hidden_gather(part)[0]()

    def give_mixed(half):
        @pl.loop(0, heads)
        def _(step):
            head = (my_head + step) % heads
            arrived(
                attended.at[span(half, chunk), span(my_tp * heads + head, width)],
                recv_o.at[head, half],
            )
        mixed_gather(half)[0]()

    for half in range(1, halves):
        for source in range(heads):
            own_queries(source, half)
        later_all(half)

    @pl.when(my_group == 0)
    def _():
        for half in range(halves):
            give_mixed(half)

    for part in range(parts):
        hidden_gather(part)[1]()

    def merge(half):
        @pl.when(my_group > 0)
        def _():
            @pl.loop(0, heads)
            def _(source):
                @pl.loop(0, my_group)
                def _(group):
                    place = source * halves + half
                    arrived(got_buf.at[group, source, half], recv_p.at[group, place])
                    arrived(got_lse.at[group, source, half], recv_l.at[group, place])
                    line = got_lse[group, source, half][:1, :]
                    theirs = jnp.broadcast_to(line, (width, chunk)).T
                    mine = own_lse[source, half]
                    top = jnp.maximum(mine, theirs)
                    a, b = jnp.exp2(mine - top), jnp.exp2(theirs - top)
                    total = a + b
                    own_buf[source, half] = (
                        own_buf[source, half] * a
                        + got_buf[group, source, half].astype(jnp.float32) * b
                    ) / total
                    own_lse[source, half] = top + jnp.log(total) * LOG2E

                o_buf[source, half] = own_buf[source, half].astype(o_buf.dtype)
                give(source, half)

    merge(0)

    def mix(half):
        mixed_gather(half)[1]()
        mixed_gather(half)[2]()
        lines = span(half, chunk)
        mixed_ref[lines, :] = jnp.dot(
            attended[lines, :], wo[...], preferred_element_type=jnp.float32
        ).astype(mixed_ref.dtype)

    for part in range(parts):
        hidden_gather(part)[2]()
    loads[3].wait()
    tall = heads * capacity

    def return_copy(group, head):
        source = group * heads + head
        return to_ep(
            product.at[span(source, capacity), :],
            back.at[span(group * heads + my_head, capacity), :],
            send_r.at[source], recv_r.at[group * heads + my_head], base + head,
        )

    def down(group):
        lines = span(group, tall)
        product[lines, :] = jnp.dot(
            hidden[lines, :], wd[...], preferred_element_type=jnp.float32
        ).astype(product.dtype)

    def hand_back(group):
        mine = span(group * heads + my_head, capacity)
        pltpu.make_async_copy(
            product.at[mine, :], back.at[mine, :], recv_r.at[group * heads + my_head]
        ).start()
        for step in range(1, heads):
            return_copy(group, (my_head + step) % heads).start()

    def combined(group):
        for step in range(heads):
            place = group * heads + (my_head + step) % heads
            arrived(back.at[span(place, capacity), :], recv_r.at[place])
        lines = span(group, tall)
        return jnp.dot(
            comb_hi[group], back[lines, :], preferred_element_type=jnp.float32
        ) + jnp.dot(comb_lo[group], back[lines, :], preferred_element_type=jnp.float32)

    def sum_copy(group):
        return to_ep(
            sums_out.at[group], sums_in.at[my_group], send_c.at[group], recv_c.at[my_group],
            group * heads + my_head,
        )

    for group in others:
        down(group)
        hand_back(group)
    down(my_group)

    for half in range(1, halves):
        merge(half)

    @pl.when(my_group > 0)
    def _():
        give_mixed(0)


    for group in others:
        sums_out[group] = combined(group).astype(sums_out.dtype)
        sum_copy(group).start()

    hand_back(my_group)

    @pl.when(my_group > 0)
    def _():
        for half in range(1, halves):
            give_mixed(half)


    loads[4].wait()
    for half in range(halves):
        mix(half)

    expert_sum = combined(my_group)
    for group in others:
        arrived(sums_in.at[group], recv_c.at[group])
        expert_sum = expert_sum + sums_in[group].astype(jnp.float32)
    expert_ref[...] = expert_sum.astype(expert_ref.dtype)

    token_gather[3]()

    @pl.loop(1, heads)
    def _(step):
        head = (my_head + step) % heads
        for copy in kv_copies(head):
            copy.wait_send()
        for half in range(halves):
            q_copy(my_group, head, half).wait_send()
            back_copy(head, half).wait_send()

    @pl.loop(0, my_group)
    def _(group):
        @pl.loop(0, heads)
        def _(head):
            for half in range(halves):
                q_copy(group, head, half).wait_send()

    @pl.loop(base + heads, n)
    def _(i):
        for half in range(halves):
            for copy in part_copies(i, half):
                copy.wait_send()

    @pl.loop(1, n)
    def _(step):
        leave_copy((me + step) % n).wait_send()

    for group in [my_group, *others]:
        for step in range(1, heads):
            return_copy(group, (my_head + step) % heads).wait_send()
    for group in others:
        sum_copy(group).wait_send()
        for copy in route_copies(group):
            copy.wait_send()

    @pl.loop(0, n)
    def _(source):
        spread(source)[3]()

    for part in range(parts):
        hidden_gather(part)[3]()

    for half in range(halves):
        mixed_gather(half)[3]()


def fused(
    cores, queries, key_rows, values, forget_log, out_weight, expert_input, norm_gain, route_ids,
    route_weights, gate_weight, up_weight, down_weight,
):
    n, tp = lax.axis_size("ep"), lax.axis_size("tp")
    rows, heads = queries.shape[0], forget_log.shape[1]
    width = queries.shape[1] // heads
    groups, halves, parts = n // heads, 2, 2
    chunk = rows // halves
    tokens, depth = expert_input.shape
    block_rows, chosen = route_ids.shape
    capacity = block_rows * chosen * 2 // n
    share = capacity // tp
    slots = n * capacity
    inner, out_width = gate_weight.shape[2], out_weight.shape[1]
    half_type, wide = jnp.bfloat16, jnp.float32
    vmem, hbm = pl.BlockSpec(memory_space=pltpu.VMEM), pl.BlockSpec(memory_space=pl.ANY)
    dma = pltpu.SemaphoreType.DMA
    blocks = n * n // 2
    return pl.pallas_call(
        functools.partial(fused_kernel, n, tp, heads, cores),
        out_shape=(
            jax.ShapeDtypeStruct((rows, out_width), half_type),
            jax.ShapeDtypeStruct((block_rows, out_width), half_type),
        ),
        in_specs=[hbm, hbm, hbm, vmem, hbm, vmem, vmem, vmem, hbm, hbm, hbm, hbm],
        out_specs=(vmem, vmem),
        scratch_shapes=[
            pltpu.VMEM((depth, inner), half_type), pltpu.VMEM((depth, inner), half_type),
            pltpu.VMEM((inner * tp, out_width), half_type),
            pltpu.VMEM((width * heads * tp, out_width), half_type),
            pltpu.VMEM((tokens, depth), half_type), pltpu.VMEM((block_rows, depth), half_type),
            pltpu.VMEM((n * share, depth), half_type), pltpu.VMEM((slots, depth), half_type),
            pltpu.VMEM((slots, inner * tp), half_type), pltpu.VMEM((slots, out_width), half_type),
            pltpu.VMEM((slots, out_width), half_type),
            pltpu.VMEM((groups, block_rows, heads * capacity), half_type),
            pltpu.VMEM((groups, block_rows, heads * capacity), half_type),
            pltpu.VMEM((groups, chosen, block_rows), jnp.int32),
            pltpu.VMEM((groups, chosen, block_rows), wide),
            pltpu.VMEM((groups, block_rows, out_width), half_type),
            pltpu.VMEM((groups, block_rows, out_width), half_type),
            pltpu.VMEM((heads * rows, 2 * width), half_type),
            pltpu.VMEM((heads * rows, 2 * width), half_type),
            pltpu.VMEM((n, halves, chunk, 2 * width), half_type),
            pltpu.VMEM((heads, halves, chunk, width), half_type),
            pltpu.VMEM((heads, halves, chunk, width), wide),
            pltpu.VMEM((heads, halves, chunk, width), wide),
            pltpu.VMEM((n, halves, chunk, width), half_type),
            pltpu.VMEM((n, halves, 8, chunk), wide),
            pltpu.VMEM((groups, heads, halves, chunk, width), half_type),
            pltpu.VMEM((groups, heads, halves, 8, chunk), wide),
            pltpu.VMEM((rows, width * heads * tp), half_type),
            dma((5,)), dma((heads,)), dma((heads,)), dma((heads,)), dma((heads,)),
            dma((n, halves)), dma((n, halves)), dma((heads, halves)), dma((heads, halves)),
            dma((n, halves)), dma((groups, heads * halves)),
            dma((n, halves)), dma((groups, heads * halves)),
            dma((tp, tp)), dma((tp,)), dma((n,)), dma((n,)), dma((n * tp, tp)), dma((n * tp,)),
            dma((parts * tp, tp)), dma((parts * tp,)), dma((n,)), dma((n,)),
            dma((halves * tp, tp)), dma((halves * tp,)),
            dma((groups,)), dma((groups,)), dma((groups,)), dma((groups,)), dma((groups,)), dma((groups,)),
        ],
        compiler_params=pltpu.CompilerParams(
            collective_id=0, has_side_effects=True, vmem_limit_bytes=58 * 1024 * 1024
        ),
        cost_estimate=pl.CostEstimate(
            flops=6 * slots * depth * inner + 2 * rows * rows * width * blocks,
            bytes_accessed=8 * depth * inner, transcendentals=blocks * rows * rows,
        ),
    )(
        queries, key_rows, values, forget_log.T, expert_input, norm_gain.reshape(1, depth),
        route_ids.T, route_weights.T, gate_weight, up_weight, down_weight, out_weight,
    )


def chip_cores(mesh):
    names = list(mesh.axis_names)
    line = mesh.devices.transpose(names.index("ep"), names.index("tp"))[0]
    spots = [getattr(device, "coords", i) for i, device in enumerate(line)]
    spots = [tuple(spot) if hasattr(spot, "__len__") else spot for spot in spots]
    cores = sum(spot == spots[0] for spot in spots)
    even = len(spots) % cores == 0 and all(
        spots[i] == spots[i - i % cores] for i in range(len(spots))
    )
    return cores if even else 1


def fits(n, tp, heads, block_rows, chosen, local_experts, inner):
    capacity = block_rows * chosen * 2 // (n * local_experts)
    return (
        local_experts == 1 and n % heads == 0 and heads > 1 and capacity % (16 * tp) == 0
        and n % 2 == 0 and inner % 256 == 0
    )


def choose(cores, *args):
    n, tp = lax.axis_size("ep"), lax.axis_size("tp")
    ids, gate_weight = args[7], args[9]
    if fits(
        n, tp, args[3].shape[1], ids.shape[0], ids.shape[1], gate_weight.shape[0],
        gate_weight.shape[2],
    ):
        return fused(cores, *args)
    return staged(*args)


def solution(mesh):
    placed = (
        P("ep", "tp"),
        P("ep", "tp"),
        P("ep", "tp"),
        P(None, "tp"),
        P(None, "tp"),
        P(("ep", "tp"), None),
        P(),
        P("ep", None),
        P("ep", None),
        P("ep", None, "tp"),
        P("ep", None, "tp"),
        P("ep", None, "tp"),
    )
    return jax.shard_map(
        functools.partial(choose, chip_cores(mesh)), mesh=mesh, in_specs=placed,
        out_specs=(P("ep", "tp"), P("ep", "tp")), check_vma=False,
    )
```

```python
import functools
import math

import jax
import jax.numpy as jnp
from jax import lax
from jax.experimental import pallas as pl
from jax.experimental.pallas import tpu as pltpu
from jax.sharding import PartitionSpec as P

EPSILON = 1e-05
LOG2E = math.log2(math.e)


def attention_kernel(
    n, tp, heads, gate_row, gate_col, q_ref, k_ref, v_ref, pick_ref, token_ref,
    out_ref, routed_ref,
    k_buf, v_buf, q_buf, o_buf, token_buf, leave_buf,
    recv_k, recv_v, recv_q, recv_o, send_k, send_v, send_q, send_o, pass_k, pass_v,
    send_t, recv_t, send_a, recv_a, send_f, recv_f,
):
    members = n // heads
    rows = k_ref.shape[0]
    width = k_ref.shape[1] // heads
    chunk = rows // members
    me = lax.axis_index("ep")
    my_member = me % members
    my_head = me // members
    my_tp = lax.axis_index("tp")
    tokens = token_ref.shape[0]

    barrier = pltpu.get_barrier_semaphore()

    @pl.loop(1, n)
    def _(step):
        pl.semaphore_signal(barrier, inc=1, device_id={"ep": (me + step) % n})

    @pl.loop(1, tp)
    def _(step):
        pl.semaphore_signal(barrier, inc=1, device_id={"tp": (my_tp + step) % tp})

    pl.semaphore_wait(barrier, n + tp - 2)

    def k_copy(target, head):
        cols = pl.ds(pl.multiple_of(head * width, width), width)
        return pltpu.make_async_remote_copy(
            src_ref=k_ref.at[:, cols], dst_ref=k_buf.at[me], send_sem=send_k.at[head],
            recv_sem=recv_k.at[me], device_id={"ep": target},
        )

    def v_copy(target, head):
        cols = pl.ds(pl.multiple_of(head * width, width), width)
        return pltpu.make_async_remote_copy(
            src_ref=v_ref.at[:, cols], dst_ref=v_buf.at[me], send_sem=send_v.at[head],
            recv_sem=recv_v.at[me], device_id={"ep": target},
        )

    def q_copy(target):
        cols = pl.ds(pl.multiple_of((target // members) * width, width), width)
        part = pl.ds(pl.multiple_of((target % members) * chunk, chunk), chunk)
        return pltpu.make_async_remote_copy(
            src_ref=q_ref.at[part, cols], dst_ref=q_buf.at[me], send_sem=send_q.at[target],
            recv_sem=recv_q.at[me], device_id={"ep": target},
        )

    def pass_copies(source, target):
        return (
            pltpu.make_async_remote_copy(
                src_ref=k_buf.at[source], dst_ref=k_buf.at[source],
                send_sem=pass_k.at[source, target % members],
                recv_sem=recv_k.at[source], device_id={"ep": target},
            ),
            pltpu.make_async_remote_copy(
                src_ref=v_buf.at[source], dst_ref=v_buf.at[source],
                send_sem=pass_v.at[source, target % members],
                recv_sem=recv_v.at[source], device_id={"ep": target},
            ),
        )

    def back_copy(source):
        cols = pl.ds(pl.multiple_of(my_head * width, width), width)
        part = pl.ds(pl.multiple_of(my_member * chunk, chunk), chunk)
        return pltpu.make_async_remote_copy(
            src_ref=o_buf.at[source], dst_ref=out_ref.at[part, cols], send_sem=send_o.at[source],
            recv_sem=recv_o.at[me], device_id={"ep": source},
        )

    def token_spot(owner):
        return token_buf.at[pl.ds(pl.multiple_of(owner * tokens, tokens), tokens), :]

    def token_copy(target):
        return pltpu.make_async_remote_copy(
            src_ref=token_ref, dst_ref=token_spot(my_tp), send_sem=send_t.at[target],
            recv_sem=recv_t.at[my_tp], device_id={"tp": target},
        )

    def leave_copy(target):
        return pltpu.make_async_remote_copy(
            src_ref=leave_buf.at[target], dst_ref=routed_ref.at[me, my_tp],
            send_sem=send_a.at[target], recv_sem=recv_a.at[me], device_id={"ep": target},
        )

    def spread_copy(source, target):
        spot = routed_ref.at[source, my_tp]
        return pltpu.make_async_remote_copy(
            src_ref=spot, dst_ref=spot, send_sem=send_f.at[source, target],
            recv_sem=recv_f.at[source, my_tp], device_id={"tp": target},
        )

    pltpu.make_async_copy(token_ref, token_spot(my_tp), recv_t.at[my_tp]).start()

    @pl.loop(1, tp)
    def _(step):
        token_copy((my_tp + step) % tp).start()

    own_cols = pl.ds(pl.multiple_of(my_head * width, width), width)
    own_part = pl.ds(pl.multiple_of(my_member * chunk, chunk), chunk)
    pltpu.make_async_copy(k_ref.at[:, own_cols], k_buf.at[me], recv_k.at[me]).start()
    pltpu.make_async_copy(v_ref.at[:, own_cols], v_buf.at[me], recv_v.at[me]).start()
    pltpu.make_async_copy(q_ref.at[own_part, own_cols], q_buf.at[me], recv_q.at[me]).start()

    @pl.loop(1, heads)
    def _(step):
        head = (my_head + step) % heads
        k_copy(head * members + my_member, head).start()
        v_copy(head * members + my_member, head).start()

    @pl.loop(1, n)
    def _(step):
        q_copy((me + step) % n).start()

    @pl.loop(0, tp)
    def _(owner):
        pltpu.make_async_copy(token_spot(owner), token_spot(owner), recv_t.at[owner]).wait()

    @pl.loop(0, n)
    def _(target):
        leave_buf[target] = jnp.dot(
            pick_ref[target], token_buf[...], preferred_element_type=jnp.float32
        ).astype(leave_buf.dtype)

    pltpu.make_async_copy(leave_buf.at[me], routed_ref.at[me, my_tp], recv_a.at[me]).start()

    @pl.loop(1, n)
    def _(step):
        leave_copy((me + step) % n).start()

    def landed(source):
        pltpu.make_async_copy(k_buf.at[source], k_buf.at[source], recv_k.at[source]).wait()
        pltpu.make_async_copy(v_buf.at[source], v_buf.at[source], recv_v.at[source]).wait()

    @pl.loop(0, heads)
    def _(step):
        source = ((my_head + step) % heads) * members + my_member
        landed(source)

        @pl.loop(1, members)
        def _(other):
            for copy in pass_copies(source, my_head * members + (my_member + other) % members):
                copy.start()

    column = lax.broadcasted_iota(jnp.int32, (chunk, rows), 1)
    line = lax.broadcasted_iota(jnp.int32, (chunk, rows), 0) + my_member * chunk
    causal = column <= line
    factor = LOG2E * width ** (-0.5)

    @pl.loop(0, n)
    def _(i):
        pltpu.make_async_copy(q_buf.at[i], q_buf.at[i], recv_q.at[i]).wait()

        @pl.when(i % members != my_member)
        def _():
            landed(i)

        query = q_buf[i]
        line_gate = gate_col[i]

        def scores_of(j):
            raw = lax.dot_general(
                query, k_buf[j], (((1,), (1,)), ((), ())), preferred_element_type=jnp.float32
            )
            return raw * factor + (line_gate - gate_row[j])

        def weigh(weights, j):
            return jnp.dot(
                weights.astype(jnp.bfloat16), v_buf[j], preferred_element_type=jnp.float32
            )

        scores = jnp.where(causal, scores_of(i), -jnp.inf)
        top = jnp.max(scores, axis=1, keepdims=True)
        weights = jnp.exp2(scores - top)
        total = jnp.sum(weights, axis=1, keepdims=True)
        held = weigh(weights, i)

        def fold(j, state):
            top, total, held = state
            scores = scores_of(j)
            newest = jnp.maximum(top, jnp.max(scores, axis=1, keepdims=True))
            shrink = jnp.exp2(top - newest)
            weights = jnp.exp2(scores - newest)
            total = total * shrink + jnp.sum(weights, axis=1, keepdims=True)
            held = held * shrink + weigh(weights, j)
            return newest, total, held

        top, total, held = lax.fori_loop(0, i, fold, (top, total, held))
        o_buf[i] = (held / total).astype(o_buf.dtype)

        @pl.when(i != me)
        def _():
            back_copy(i).start()

        source = (me + n - i) % n
        spot = routed_ref.at[source, my_tp]
        pltpu.make_async_copy(spot, spot, recv_a.at[source]).wait()

        @pl.loop(1, tp)
        def _(step):
            spread_copy(source, (my_tp + step) % tp).start()

    own = pltpu.make_async_copy(o_buf.at[me], out_ref.at[own_part, own_cols], recv_o.at[me])
    own.start()

    @pl.loop(1, heads)
    def _(step):
        head = (my_head + step) % heads
        k_copy(head * members + my_member, head).wait_send()
        v_copy(head * members + my_member, head).wait_send()

    @pl.loop(1, n)
    def _(step):
        q_copy((me + step) % n).wait_send()
        back_copy((me + step) % n).wait_send()
        leave_copy((me + step) % n).wait_send()

    @pl.loop(1, tp)
    def _(step):
        token_copy((my_tp + step) % tp).wait_send()

    @pl.loop(0, n)
    def _(source):
        @pl.loop(1, tp)
        def _(step):
            other = (my_tp + step) % tp
            spread_copy(source, other).wait_send()
            spot = routed_ref.at[source, other]
            pltpu.make_async_copy(spot, spot, recv_f.at[source, other]).wait()

    @pl.loop(0, heads)
    def _(step):
        source = step * members + my_member

        @pl.loop(1, members)
        def _(other):
            for copy in pass_copies(source, my_head * members + (my_member + other) % members):
                copy.wait_send()

    @pl.loop(0, n)
    def _(i):
        cols = pl.ds(pl.multiple_of((i // members) * width, width), width)
        part = pl.ds(pl.multiple_of((i % members) * chunk, chunk), chunk)
        spot = out_ref.at[part, cols]
        pltpu.make_async_copy(spot, spot, recv_o.at[i]).wait()


def attention(queries, key_rows, values, forget_log, picks, normed):
    n, tp = lax.axis_size("ep"), lax.axis_size("tp")
    share, depth = picks.shape[1], normed.shape[1]
    rows, heads = queries.shape[0], forget_log.shape[1]
    width = queries.shape[1] // heads
    members = n // heads
    chunk = rows // members
    me = lax.axis_index("ep")
    gates = lax.dynamic_slice_in_dim(forget_log.T * LOG2E, me // members, 1, 0)
    gate_row = gates.reshape(n, 1, rows)
    gate_col = lax.dynamic_slice_in_dim(
        gates.reshape(n, members, chunk), me % members, 1, 1
    ).reshape(n, chunk, 1)
    vmem = pl.BlockSpec(memory_space=pltpu.VMEM)
    dma = pltpu.SemaphoreType.DMA
    blocks = n * (n + 1) // 2
    return pl.pallas_call(
        functools.partial(attention_kernel, n, tp, heads),
        out_shape=(
            jax.ShapeDtypeStruct((rows, heads * width), jnp.bfloat16),
            jax.ShapeDtypeStruct((n, tp, share, depth), jnp.bfloat16),
        ),
        in_specs=[vmem] * 7,
        out_specs=(vmem, vmem),
        scratch_shapes=[
            pltpu.VMEM((n, rows, width), jnp.bfloat16),
            pltpu.VMEM((n, rows, width), jnp.bfloat16),
            pltpu.VMEM((n, chunk, width), jnp.bfloat16),
            pltpu.VMEM((n, chunk, width), jnp.bfloat16),
            pltpu.VMEM((tp * normed.shape[0], depth), jnp.bfloat16),
            pltpu.VMEM((n, share, depth), jnp.bfloat16),
            dma((n,)), dma((n,)), dma((n,)), dma((n,)),
            dma((heads,)), dma((heads,)), dma((n,)), dma((n,)),
            dma((n, members)), dma((n, members)),
            dma((tp,)), dma((tp,)), dma((n,)), dma((n,)), dma((n, tp)), dma((n, tp)),
        ],
        compiler_params=pltpu.CompilerParams(
            collective_id=0, has_side_effects=True, vmem_limit_bytes=40 * 1024 * 1024
        ),
        cost_estimate=pl.CostEstimate(
            flops=40 * blocks * chunk * rows * width, bytes_accessed=8 * rows * heads * width,
            transcendentals=blocks * chunk * rows,
        ),
    )(gate_row, gate_col, queries, key_rows, values, picks, normed)


def slot_places(route_rows, experts, capacity):
    entries = route_rows.reshape(-1)
    matches = (entries[:, None] == jnp.arange(experts, dtype=jnp.int32)[None, :]).astype(jnp.int32)
    earlier = jnp.cumsum(matches, axis=0) - matches
    ranking = jnp.sum(earlier * matches, axis=1)
    return entries * capacity + ranking


def staged(
    queries,
    key_rows,
    values,
    forget_log,
    out_weight,
    expert_input,
    norm_gain,
    route_ids,
    route_weights,
    gate_weight,
    up_weight,
    down_weight,
):
    as_float = expert_input.astype(jnp.float32)
    center = jnp.mean(as_float, axis=1, keepdims=True)
    variance = jnp.mean(jnp.square(as_float - center), axis=1, keepdims=True)
    normed = ((as_float - center) * lax.rsqrt(variance + EPSILON) * norm_gain).astype(jnp.bfloat16)
    block_rows = route_ids.shape[0]
    chosen = route_ids.shape[1]
    expert_local = gate_weight.shape[0]
    ep_count = lax.axis_size("ep")
    tp_count = lax.axis_size("tp")
    experts = expert_local * ep_count
    capacity = block_rows * chosen * 2 // experts
    places = slot_places(route_ids, experts, capacity)
    share_size = capacity // tp_count
    own_slots = lax.axis_index("tp") * share_size + jnp.arange(share_size, dtype=jnp.int32)
    part_slots = jnp.arange(experts, dtype=jnp.int32)[:, None] * capacity + own_slots[None, :]
    picks = jnp.any(
        part_slots.reshape(ep_count, expert_local * share_size)[:, :, None, None]
        == places.reshape(block_rows, chosen).T[None, None, :, :],
        axis=2,
    ).astype(jnp.bfloat16)
    attended, routed = attention(queries, key_rows, values, forget_log, picks, normed)
    arrived_rows = (
        routed.reshape(ep_count, tp_count, expert_local, share_size, routed.shape[3])
        .transpose(0, 2, 1, 3, 4)
        .reshape(ep_count, expert_local, capacity, routed.shape[3])
    )
    gate_part = jnp.einsum(
        "sxcd,xdf->sxcf", arrived_rows, gate_weight, preferred_element_type=jnp.float32
    )
    up_part = jnp.einsum(
        "sxcd,xdf->sxcf", arrived_rows, up_weight, preferred_element_type=jnp.float32
    )
    hidden = (jax.nn.silu(gate_part) * up_part).astype(jnp.bfloat16)
    slots_all = ep_count * expert_local * capacity
    flat_hidden = hidden.reshape(slots_all, hidden.shape[3])
    out_width = out_weight.shape[1]
    mixer_sum = jnp.dot(
        lax.all_gather(attended, "tp", axis=1, tiled=True),
        out_weight,
        preferred_element_type=jnp.float32,
    )
    part_rows = lax.all_gather(flat_hidden, "tp", axis=1, tiled=True)
    shaped = part_rows.reshape(ep_count, expert_local, capacity, part_rows.shape[1])
    product = jnp.einsum("sxcf,xfd->sxcd", shaped, down_weight, preferred_element_type=jnp.float32)
    expert_sum = product.reshape(slots_all, out_width)
    leaving = expert_sum.astype(jnp.bfloat16).reshape(ep_count, expert_local, capacity, out_width)
    returned = lax.all_to_all(leaving, "ep", split_axis=0, concat_axis=0, tiled=True)
    picked = jnp.take(returned.reshape(experts * capacity, out_width), places, axis=0).astype(
        jnp.float32
    )
    combined = jnp.sum(
        (picked * route_weights.reshape(-1)[:, None]).reshape(block_rows, chosen, out_width), axis=1
    )
    return (mixer_sum.astype(jnp.bfloat16), combined.astype(jnp.bfloat16))


def fused_kernel(
    n, tp, heads, cores, q_ref, k_ref, v_ref, gate_ref, x_ref, gain_ref, ids_ref, mix_ref,
    wg_ref, wu_ref, wd_ref, wo_ref,
    mixed_ref, expert_ref,
    wg, wu, wd, wo, x_buf, token_buf, leave_buf, routed, hidden, product, back, comb_hi, comb_lo,
    ids_buf, mix_buf, sums_out, sums_in,
    k_buf, v_buf, q_buf, o_buf, own_buf, own_lse, part_buf, part_lse, got_buf, got_lse, attended,
    load, send_k, recv_k, send_v, recv_v, send_q, recv_q, send_o, recv_o,
    send_p, recv_p, send_l, recv_l, send_t, recv_t, send_a, recv_a, send_f, recv_f,
    send_h, recv_h, send_r, recv_r, send_m, recv_m,
    send_i, recv_i, send_w, recv_w, send_c, recv_c,
):
    groups = n // heads
    chips = tp // cores
    rows = k_ref.shape[0]
    width = k_ref.shape[1] // heads
    halves = q_buf.shape[1]
    chunk = rows // halves
    tokens, depth = x_ref.shape
    share = leave_buf.shape[0] // n
    capacity = share * tp
    block_rows = token_buf.shape[0]
    chosen = ids_ref.shape[0]
    inner = wg.shape[1]
    out_width = wo.shape[1]
    factor = LOG2E * width ** (-0.5)
    me, my_tp = lax.axis_index("ep"), lax.axis_index("tp")
    my_group, my_head = me // heads, me % heads
    my_chip, my_core = my_tp // cores, my_tp % cores
    base = my_group * heads

    siblings = [my_chip * cores + (my_core + s) % cores for s in range(1, cores)]
    across = [((my_chip + s) % chips) * cores + my_core for s in range(1, chips)]
    rest = [
        ((my_chip + s) % chips) * cores + (my_core + r) % cores
        for s in range(1, chips) for r in range(1, cores)
    ]

    def span(start, size):
        return pl.ds(pl.multiple_of(start * size, size), size)

    def arrived(ref, sem):
        pltpu.make_async_copy(ref, ref, sem).wait()

    def to_ep(src, dst, send, recv, target):
        return pltpu.make_async_remote_copy(
            src_ref=src, dst_ref=dst, send_sem=send, recv_sem=recv, device_id={"ep": target}
        )

    def gather(piece, sends, recvs, first):
        def copy(owner, target):
            return pltpu.make_async_remote_copy(
                src_ref=piece(owner), dst_ref=piece(owner), send_sem=sends.at[first + owner, target],
                recv_sem=recvs.at[first + owner], device_id={"tp": target},
            )

        def start():
            for target in across + siblings:
                copy(my_tp, target).start()

        def forward():
            for owner in across:
                arrived(piece(owner), recvs.at[first + owner])
                for target in siblings:
                    copy(owner, target).start()

        def finish():
            for owner in siblings + rest:
                arrived(piece(owner), recvs.at[first + owner])

        def drain():
            for target in across + siblings:
                copy(my_tp, target).wait_send()
            for owner in across:
                for target in siblings:
                    copy(owner, target).wait_send()

        return start, forward, finish, drain

    def token_piece(owner):
        return token_buf.at[span(owner, tokens), :]

    def routed_piece(source):
        return lambda owner: routed.at[span(source * tp + owner, share), :]

    parts = send_h.shape[0] // tp
    strip = inner // parts

    def hidden_piece(part):
        return lambda owner: hidden.at[:, span(owner * parts + part, strip)]

    def mixed_piece(half):
        return lambda owner: attended.at[span(half, chunk), span(owner, heads * width)]

    token_gather = gather(token_piece, send_t, recv_t, 0)

    def spread(source):
        return gather(routed_piece(source), send_f, recv_f, source * tp)

    def hidden_gather(part):
        return gather(hidden_piece(part), send_h, recv_h, part * tp)

    def mixed_gather(half):
        return gather(mixed_piece(half), send_m, recv_m, half * tp)

    straight = [(heads // 2 + s) % heads for s in (*range(0, heads, 2), *range(1, heads, 2))]
    across_groups = [(g, s) for g in range(1, groups) for s in straight]
    in_group = [(0, s) for s in range(1, heads)]
    order = [(0, 0)]
    for place in range(max(len(across_groups), len(in_group))):
        order += across_groups[place : place + 1] + in_group[place : place + 1]

    def peer(step, sign):
        group, head = order[step]
        return ((my_group + groups + sign * group) % groups) * heads + (
            my_head + heads + sign * head
        ) % heads

    loads = [
        pltpu.make_async_copy(src, dst, load.at[i])
        for i, (src, dst) in enumerate((
            (x_ref, x_buf), (wg_ref.at[0], wg), (wu_ref.at[0], wu), (wd_ref.at[0], wd), (wo_ref, wo),
        ))
    ]
    loads[0].start()

    barrier = pltpu.get_barrier_semaphore()

    @pl.loop(1, n)
    def _(step):
        pl.semaphore_signal(barrier, inc=1, device_id={"ep": (me + step) % n})

    @pl.loop(1, tp)
    def _(step):
        pl.semaphore_signal(barrier, inc=1, device_id={"tp": (my_tp + step) % tp})

    loads[0].wait()
    as_float = x_buf[...].astype(jnp.float32)
    center = jnp.mean(as_float, axis=1, keepdims=True)
    shifted = as_float - center
    variance = jnp.mean(jnp.square(shifted), axis=1, keepdims=True)
    token_buf[span(my_tp, tokens), :] = (
        shifted * lax.rsqrt(variance + EPSILON) * gain_ref[...]
    ).astype(token_buf.dtype)

    ids_buf[my_group] = ids_ref[...]
    mix_buf[my_group] = mix_ref[...]
    pl.semaphore_wait(barrier, n + tp - 2)
    token_gather[0]()
    others = [(my_group + step) % groups for step in range(1, groups)]

    def route_copies(group):
        target = group * heads + my_head
        return (
            to_ep(ids_ref, ids_buf.at[my_group], send_i.at[group], recv_i.at[my_group], target),
            to_ep(mix_ref, mix_buf.at[my_group], send_w.at[group], recv_w.at[my_group], target),
        )

    for group in others:
        for copy in route_copies(group):
            copy.start()

    def k_spot(source):
        return k_buf.at[span(source, rows), :width]

    def v_spot(source):
        return v_buf.at[span(source, rows), :width]

    def q_spot(source, half):
        return q_buf.at[source, half, :, :width]

    def kv_copies(head):
        cols = span(head, width)
        target = base + head
        return (
            to_ep(k_ref.at[:, cols], k_spot(my_head), send_k.at[head], recv_k.at[my_head], target),
            to_ep(v_ref.at[:, cols], v_spot(my_head), send_v.at[head], recv_v.at[my_head], target),
        )

    def q_copy(group, head, half):
        target = group * heads + head
        return to_ep(
            q_ref.at[span(half, chunk), span(head, width)], q_spot(me, half),
            send_q.at[target, half], recv_q.at[me, half], target,
        )

    own_cols = span(my_head, width)
    keep_k = pltpu.make_async_copy(k_ref.at[:, own_cols], k_spot(my_head), recv_k.at[my_head])
    keep_v = pltpu.make_async_copy(v_ref.at[:, own_cols], v_spot(my_head), recv_v.at[my_head])
    keep_k.start()
    keep_v.start()
    for half in range(halves):
        pltpu.make_async_copy(
            q_ref.at[span(half, chunk), own_cols], q_spot(me, half), recv_q.at[me, half]
        ).start()

    def lower_queries(half):
        @pl.loop(0, my_group)
        def _(group):
            @pl.loop(0, heads)
            def _(step):
                q_copy(group, (my_head + step) % heads, half).start()

    @pl.loop(1, heads)
    def _(step):
        for copy in kv_copies((my_head + step) % heads):
            copy.start()

    lower_queries(0)

    terms = lax.broadcasted_iota(jnp.int32, (width, chunk), 0)

    def gate_columns(block, sign, offset):
        gate = gate_ref[pl.ds(my_head, 1), span(block, chunk)] * (sign * width**0.5)
        table = jnp.where((terms >= 3 - offset) & (terms < 6 - offset), 1.0, 0.0)
        for place in range(offset, offset + 3):
            piece = gate.astype(jnp.bfloat16).astype(jnp.float32)
            gate = gate - piece
            table = jnp.where(terms == place, piece, table)
        return table.T.astype(jnp.bfloat16)

    v_buf[:, width:] = jnp.ones((heads * rows, width), v_buf.dtype)

    @pl.loop(0, heads * halves)
    def _(place):
        k_buf[span(place, chunk), width:] = gate_columns(base * halves + place, -1.0, 3)

    @pl.loop(base, n)
    def _(i):
        for half in range(halves):
            q_buf[i, half, :, width:] = gate_columns(i * halves + half, 1.0, 0)

    def group_queries(half):
        @pl.loop(1, heads)
        def _(step):
            q_copy(my_group, (my_head + step) % heads, half).start()

    group_queries(0)

    for copy in loads[1:]:
        copy.start()

    before = lax.broadcasted_iota(jnp.int32, (block_rows, block_rows), 0)
    after = lax.broadcasted_iota(jnp.int32, (block_rows, block_rows), 1)
    earlier = jnp.where(before < after, 1.0, 0.0).astype(jnp.bfloat16)

    def places(ids, first, count):
        expert = lax.broadcasted_iota(jnp.int32, (count, block_rows), 0) + first
        matches = [expert == ids[k : k + 1, :] for k in range(chosen)]
        named = functools.reduce(jnp.logical_or, matches)
        ranks = jnp.dot(
            jnp.where(named, 1.0, 0.0).astype(jnp.bfloat16), earlier,
            preferred_element_type=jnp.float32,
        )
        return matches, jnp.where(named, ranks, -1.0)

    def per_slot(table, count):
        return jnp.broadcast_to(table[:, None, :], (table.shape[0], count, block_rows))

    slots = lax.broadcasted_iota(jnp.int32, (n, share, block_rows), 1) + my_tp * share
    picks = jnp.where(
        per_slot(places(ids_ref[...], 0, n)[1], share) == slots.astype(jnp.float32), 1.0, 0.0
    ).reshape(n * share, block_rows).astype(jnp.bfloat16)

    token_gather[1]()
    token_gather[2]()

    piece = depth // 8

    @pl.loop(0, depth // piece)
    def _(i):
        cols = span(i, piece)
        leave_buf[:, cols] = jnp.dot(
            picks, token_buf[:, cols], preferred_element_type=jnp.float32
        ).astype(leave_buf.dtype)

    def leave_copy(target):
        return to_ep(
            leave_buf.at[span(target, share), :], routed_piece(me)(my_tp),
            send_a.at[target], recv_a.at[me], target,
        )

    pltpu.make_async_copy(
        leave_buf.at[span(me, share), :], routed_piece(me)(my_tp), recv_a.at[me]
    ).start()

    for step in range(1, n):
        leave_copy(peer(step, 1)).start()

    for half in range(1, halves):
        group_queries(half)
        lower_queries(half)

    def combining(group):
        matches, ranks = places(ids_buf[group], base, heads)
        scale = functools.reduce(
            jnp.add,
            [
                jnp.where(match, mix_buf[group, k : k + 1, :], 0.0)
                for k, match in enumerate(matches)
            ],
        )
        all_slots = lax.broadcasted_iota(jnp.int32, (heads, capacity, block_rows), 1)
        comb = jnp.where(
            per_slot(ranks, capacity) == all_slots.astype(jnp.float32),
            per_slot(scale, capacity), 0.0,
        ).reshape(heads * capacity, block_rows).T
        high = comb.astype(jnp.bfloat16)
        comb_hi[group] = high
        comb_lo[group] = (comb - high.astype(jnp.float32)).astype(jnp.bfloat16)

    combining(my_group)
    for group in others:
        arrived(ids_buf.at[group], recv_i.at[group])
        arrived(mix_buf.at[group], recv_w.at[group])
        combining(group)

    @pl.loop(0, heads)
    def _(step):
        source = (my_head + step) % heads
        arrived(k_spot(source), recv_k.at[source])
        arrived(v_spot(source), recv_v.at[source])

    stretch = 2 * chunk

    def attend(i, half, keys, causal):
        query = q_buf[i, half]

        def scores_of(lines):
            return lax.dot_general(
                query, k_buf[lines, :], (((1,), (1,)), ((), ())), preferred_element_type=jnp.float32
            )

        open_keys = keys - chunk if causal else keys
        cuts = [
            slice(cut, min(cut + stretch, open_keys)) for cut in range(0, open_keys, stretch)
        ]
        if causal:
            cuts = [slice(open_keys, keys), *cuts]
        scores = scores_of(cuts[0])
        if causal:
            column = lax.broadcasted_iota(jnp.int32, (chunk, chunk), 1)
            line = lax.broadcasted_iota(jnp.int32, (chunk, chunk), 0)
            scores = jnp.where(column <= line, scores, -jnp.inf)
        top = jnp.max(scores, axis=1, keepdims=True)
        held = None
        for place, lines in enumerate(cuts):
            later = scores_of(cuts[place + 1]) if place + 1 < len(cuts) else None
            weights = jnp.exp2((scores - top) * factor).astype(jnp.bfloat16)
            gained = jnp.dot(weights, v_buf[lines, :], preferred_element_type=jnp.float32)
            held = gained if held is None else held + gained
            if later is not None:
                newest = jnp.maximum(top, jnp.max(later, axis=1, keepdims=True))
                held = held * jnp.exp2((top - newest) * factor)
                top, scores = newest, later
        total = held[:, width:]
        return held[:, :width] / total, top * factor + jnp.log(total) * LOG2E

    def back_copy(source, half):
        return to_ep(
            o_buf.at[source, half], attended.at[span(half, chunk), span(my_tp * heads + my_head, width)],
            send_o.at[source, half], recv_o.at[my_head, half], base + source,
        )

    per_head = n // heads

    def give(source, half):
        @pl.when(source != my_head)
        def _():
            back_copy(source, half).start()

        @pl.when(source == my_head)
        def _():
            pltpu.make_async_copy(
                o_buf.at[source, half],
                attended.at[span(half, chunk), span(my_tp * heads + my_head, width)],
                recv_o.at[my_head, half],
            ).start()

    def spread_step(step):
        source = peer(step, -1)
        arrived(routed_piece(source)(my_tp), recv_a.at[source])
        spread(source)[0]()

    def own_queries(source, half):
        i = base + source
        arrived(q_spot(i, half), recv_q.at[i, half])
        out, lse = attend(i, half, source * rows + (half + 1) * chunk, True)

        @pl.when(my_group == 0)
        def _():
            o_buf[source, half] = out.astype(o_buf.dtype)
            give(source, half)

        @pl.when(my_group > 0)
        def _():
            own_buf[source, half] = out
            own_lse[source, half] = lse

    def part_copies(i, half):
        slot = i % heads
        return (
            to_ep(part_buf.at[i, half], got_buf.at[my_group, slot, half],
                  send_p.at[i, half], recv_p.at[my_group, slot * halves + half],
                  (i // heads) * heads + my_head),
            to_ep(part_lse.at[i, half], got_lse.at[my_group, slot, half],
                  send_l.at[i, half], recv_l.at[my_group, slot * halves + half],
                  (i // heads) * heads + my_head),
        )

    def later_queries(group, source, half):
        @pl.when(my_group + group < groups)
        def _():
            i = (my_group + group) * heads + source
            arrived(q_spot(i, half), recv_q.at[i, half])
            out, lse = attend(i, half, heads * rows, False)
            part_buf[i, half] = out.astype(part_buf.dtype)
            part_lse[i, half] = lse.T[: part_lse.shape[2], :]
            for copy in part_copies(i, half):
                copy.start()

    def later_all(half):
        for group in range(1, groups):
            @pl.loop(0, heads)
            def _(source):
                later_queries(group, source, half)

    for step in range(n):
        spread_step(step)
        if step >= 2:
            spread(peer(step - 2, -1))[1]()
        if step < heads:
            own_queries(step, 0)
        elif step < 2 * heads:
            for group in range(1, groups):
                later_queries(group, step - heads, 0)

    for step in range(n - 2, n):
        spread(peer(step, -1))[1]()

    @pl.loop(0, n)
    def _(source):
        spread(source)[2]()

    loads[1].wait()
    loads[2].wait()
    for part in range(parts):
        cols = slice(part * strip, (part + 1) * strip)
        gate_part = jnp.dot(routed[...], wg[:, cols], preferred_element_type=jnp.float32)
        up_part = jnp.dot(routed[...], wu[:, cols], preferred_element_type=jnp.float32)
        hidden[:, span(my_tp * parts + part, strip)] = (
            gate_part / (1.0 + jnp.exp(-gate_part)) * up_part
        ).astype(hidden.dtype)
        hidden_gather(part)[0]()

    def give_mixed(half):
        @pl.loop(0, heads)
        def _(step):
            head = (my_head + step) % heads
            arrived(
                attended.at[span(half, chunk), span(my_tp * heads + head, width)],
                recv_o.at[head, half],
            )
        mixed_gather(half)[0]()

    for half in range(1, halves):
        for source in range(heads):
            own_queries(source, half)
        later_all(half)

    @pl.when(my_group == 0)
    def _():
        for half in range(halves):
            give_mixed(half)

    for part in range(parts):
        hidden_gather(part)[1]()

    def merge(half):
        @pl.when(my_group > 0)
        def _():
            @pl.loop(0, heads)
            def _(source):
                @pl.loop(0, my_group)
                def _(group):
                    place = source * halves + half
                    arrived(got_buf.at[group, source, half], recv_p.at[group, place])
                    arrived(got_lse.at[group, source, half], recv_l.at[group, place])
                    line = got_lse[group, source, half][:1, :]
                    theirs = jnp.broadcast_to(line, (width, chunk)).T
                    mine = own_lse[source, half]
                    top = jnp.maximum(mine, theirs)
                    a, b = jnp.exp2(mine - top), jnp.exp2(theirs - top)
                    total = a + b
                    own_buf[source, half] = (
                        own_buf[source, half] * a
                        + got_buf[group, source, half].astype(jnp.float32) * b
                    ) / total
                    own_lse[source, half] = top + jnp.log(total) * LOG2E

                o_buf[source, half] = own_buf[source, half].astype(o_buf.dtype)
                give(source, half)

    merge(0)

    def mix(half):
        mixed_gather(half)[1]()
        mixed_gather(half)[2]()
        lines = span(half, chunk)
        mixed_ref[lines, :] = jnp.dot(
            attended[lines, :], wo[...], preferred_element_type=jnp.float32
        ).astype(mixed_ref.dtype)

    for part in range(parts):
        hidden_gather(part)[2]()
    loads[3].wait()
    tall = heads * capacity

    def return_copy(group, head):
        source = group * heads + head
        return to_ep(
            product.at[span(source, capacity), :],
            back.at[span(group * heads + my_head, capacity), :],
            send_r.at[source], recv_r.at[group * heads + my_head], base + head,
        )

    def down(group):
        lines = span(group, tall)
        product[lines, :] = jnp.dot(
            hidden[lines, :], wd[...], preferred_element_type=jnp.float32
        ).astype(product.dtype)

    def hand_back(group):
        mine = span(group * heads + my_head, capacity)
        pltpu.make_async_copy(
            product.at[mine, :], back.at[mine, :], recv_r.at[group * heads + my_head]
        ).start()
        for step in range(1, heads):
            return_copy(group, (my_head + step) % heads).start()

    def combined(group):
        for step in range(heads):
            place = group * heads + (my_head + step) % heads
            arrived(back.at[span(place, capacity), :], recv_r.at[place])
        lines = span(group, tall)
        return jnp.dot(
            comb_hi[group], back[lines, :], preferred_element_type=jnp.float32
        ) + jnp.dot(comb_lo[group], back[lines, :], preferred_element_type=jnp.float32)

    def sum_copy(group):
        return to_ep(
            sums_out.at[group], sums_in.at[my_group], send_c.at[group], recv_c.at[my_group],
            group * heads + my_head,
        )

    for group in others:
        down(group)
        hand_back(group)
    down(my_group)

    for half in range(1, halves):
        merge(half)

    @pl.when(my_group > 0)
    def _():
        give_mixed(0)


    for group in others:
        sums_out[group] = combined(group).astype(sums_out.dtype)
        sum_copy(group).start()

    hand_back(my_group)

    @pl.when(my_group > 0)
    def _():
        for half in range(1, halves):
            give_mixed(half)


    loads[4].wait()
    for half in range(halves):
        mix(half)

    expert_sum = combined(my_group)
    for group in others:
        arrived(sums_in.at[group], recv_c.at[group])
        expert_sum = expert_sum + sums_in[group].astype(jnp.float32)
    expert_ref[...] = expert_sum.astype(expert_ref.dtype)

    token_gather[3]()

    @pl.loop(1, heads)
    def _(step):
        head = (my_head + step) % heads
        for copy in kv_copies(head):
            copy.wait_send()
        for half in range(halves):
            q_copy(my_group, head, half).wait_send()
            back_copy(head, half).wait_send()

    @pl.loop(0, my_group)
    def _(group):
        @pl.loop(0, heads)
        def _(head):
            for half in range(halves):
                q_copy(group, head, half).wait_send()

    @pl.loop(base + heads, n)
    def _(i):
        for half in range(halves):
            for copy in part_copies(i, half):
                copy.wait_send()

    @pl.loop(1, n)
    def _(step):
        leave_copy((me + step) % n).wait_send()

    for group in [my_group, *others]:
        for step in range(1, heads):
            return_copy(group, (my_head + step) % heads).wait_send()
    for group in others:
        sum_copy(group).wait_send()
        for copy in route_copies(group):
            copy.wait_send()

    @pl.loop(0, n)
    def _(source):
        spread(source)[3]()

    for part in range(parts):
        hidden_gather(part)[3]()

    for half in range(halves):
        mixed_gather(half)[3]()


def fused(
    cores, queries, key_rows, values, forget_log, out_weight, expert_input, norm_gain, route_ids,
    route_weights, gate_weight, up_weight, down_weight,
):
    n, tp = lax.axis_size("ep"), lax.axis_size("tp")
    rows, heads = queries.shape[0], forget_log.shape[1]
    width = queries.shape[1] // heads
    groups, halves, parts = n // heads, 2, 2
    chunk = rows // halves
    tokens, depth = expert_input.shape
    block_rows, chosen = route_ids.shape
    capacity = block_rows * chosen * 2 // n
    share = capacity // tp
    slots = n * capacity
    inner, out_width = gate_weight.shape[2], out_weight.shape[1]
    half_type, wide = jnp.bfloat16, jnp.float32
    vmem, hbm = pl.BlockSpec(memory_space=pltpu.VMEM), pl.BlockSpec(memory_space=pl.ANY)
    dma = pltpu.SemaphoreType.DMA
    blocks = n * n // 2
    return pl.pallas_call(
        functools.partial(fused_kernel, n, tp, heads, cores),
        out_shape=(
            jax.ShapeDtypeStruct((rows, out_width), half_type),
            jax.ShapeDtypeStruct((block_rows, out_width), half_type),
        ),
        in_specs=[hbm, hbm, hbm, vmem, hbm, vmem, vmem, vmem, hbm, hbm, hbm, hbm],
        out_specs=(vmem, vmem),
        scratch_shapes=[
            pltpu.VMEM((depth, inner), half_type), pltpu.VMEM((depth, inner), half_type),
            pltpu.VMEM((inner * tp, out_width), half_type),
            pltpu.VMEM((width * heads * tp, out_width), half_type),
            pltpu.VMEM((tokens, depth), half_type), pltpu.VMEM((block_rows, depth), half_type),
            pltpu.VMEM((n * share, depth), half_type), pltpu.VMEM((slots, depth), half_type),
            pltpu.VMEM((slots, inner * tp), half_type), pltpu.VMEM((slots, out_width), half_type),
            pltpu.VMEM((slots, out_width), half_type),
            pltpu.VMEM((groups, block_rows, heads * capacity), half_type),
            pltpu.VMEM((groups, block_rows, heads * capacity), half_type),
            pltpu.VMEM((groups, chosen, block_rows), jnp.int32),
            pltpu.VMEM((groups, chosen, block_rows), wide),
            pltpu.VMEM((groups, block_rows, out_width), half_type),
            pltpu.VMEM((groups, block_rows, out_width), half_type),
            pltpu.VMEM((heads * rows, 2 * width), half_type),
            pltpu.VMEM((heads * rows, 2 * width), half_type),
            pltpu.VMEM((n, halves, chunk, 2 * width), half_type),
            pltpu.VMEM((heads, halves, chunk, width), half_type),
            pltpu.VMEM((heads, halves, chunk, width), wide),
            pltpu.VMEM((heads, halves, chunk, width), wide),
            pltpu.VMEM((n, halves, chunk, width), half_type),
            pltpu.VMEM((n, halves, 8, chunk), wide),
            pltpu.VMEM((groups, heads, halves, chunk, width), half_type),
            pltpu.VMEM((groups, heads, halves, 8, chunk), wide),
            pltpu.VMEM((rows, width * heads * tp), half_type),
            dma((5,)), dma((heads,)), dma((heads,)), dma((heads,)), dma((heads,)),
            dma((n, halves)), dma((n, halves)), dma((heads, halves)), dma((heads, halves)),
            dma((n, halves)), dma((groups, heads * halves)),
            dma((n, halves)), dma((groups, heads * halves)),
            dma((tp, tp)), dma((tp,)), dma((n,)), dma((n,)), dma((n * tp, tp)), dma((n * tp,)),
            dma((parts * tp, tp)), dma((parts * tp,)), dma((n,)), dma((n,)),
            dma((halves * tp, tp)), dma((halves * tp,)),
            dma((groups,)), dma((groups,)), dma((groups,)), dma((groups,)), dma((groups,)), dma((groups,)),
        ],
        compiler_params=pltpu.CompilerParams(
            collective_id=0, has_side_effects=True, vmem_limit_bytes=58 * 1024 * 1024
        ),
        cost_estimate=pl.CostEstimate(
            flops=6 * slots * depth * inner + 2 * rows * rows * width * blocks,
            bytes_accessed=8 * depth * inner, transcendentals=blocks * rows * rows,
        ),
    )(
        queries, key_rows, values, forget_log.T, expert_input, norm_gain.reshape(1, depth),
        route_ids.T, route_weights.T, gate_weight, up_weight, down_weight, out_weight,
    )


def chip_cores(mesh):
    names = list(mesh.axis_names)
    line = mesh.devices.transpose(names.index("ep"), names.index("tp"))[0]
    spots = [getattr(device, "coords", i) for i, device in enumerate(line)]
    spots = [tuple(spot) if hasattr(spot, "__len__") else spot for spot in spots]
    cores = sum(spot == spots[0] for spot in spots)
    even = len(spots) % cores == 0 and all(
        spots[i] == spots[i - i % cores] for i in range(len(spots))
    )
    return cores if even else 1


def fits(n, tp, heads, block_rows, chosen, local_experts, inner):
    capacity = block_rows * chosen * 2 // (n * local_experts)
    return (
        local_experts == 1 and n % heads == 0 and heads > 1 and capacity % (16 * tp) == 0
        and n % 2 == 0 and inner % 256 == 0
    )


def choose(cores, *args):
    n, tp = lax.axis_size("ep"), lax.axis_size("tp")
    ids, gate_weight = args[7], args[9]
    if fits(
        n, tp, args[3].shape[1], ids.shape[0], ids.shape[1], gate_weight.shape[0],
        gate_weight.shape[2],
    ):
        return fused(cores, *args)
    return staged(*args)


def solution(mesh):
    placed = (
        P("ep", "tp"),
        P("ep", "tp"),
        P("ep", "tp"),
        P(None, "tp"),
        P(None, "tp"),
        P(("ep", "tp"), None),
        P(),
        P("ep", None),
        P("ep", None),
        P("ep", None, "tp"),
        P("ep", None, "tp"),
        P("ep", None, "tp"),
    )
    return jax.shard_map(
        functools.partial(choose, chip_cores(mesh)), mesh=mesh, in_specs=placed,
        out_specs=(P("ep", "tp"), P("ep", "tp")), check_vma=False,
    )
```
